32 devices in a mesh: ep: 8 (over z, y), tp: 4 (over x, core).
Axes of the slice: x: 2, y: 2, z: 4, core: 2. Of those that a mesh axis runs over, the one named last changes fastest.
Arguments:
- queries: bfloat16 [8192, 1024], P('ep', 'tp'), may hold values from -6 to 6
- keys: bfloat16 [8192, 1024], P('ep', 'tp'), may hold values from -6 to 6
- values: bfloat16 [8192, 2048], P('ep', 'tp'), may hold values from -6 to 6
- log_input_gate: float32 [8192, 8], P('ep', 'tp'), may hold values from -6 to 103
- forget_preactivation: float32 [8192, 8], P('ep', 'tp'), may hold values from 0 to 16
- forget_offset: float32 [8192, 8], P('ep', 'tp'), may hold values from -0.7 to 0
- head_norm_scale: float32 [2048], P('tp'), may hold values from 0.1 to 1.9
- memory_output_weight: bfloat16 [2048, 4096], P('tp'), may hold values from -0.125 to 0.125
- second_micro_tokens: bfloat16 [4096, 4096], P('ep'), may hold values from -6 to 6
- expert_norm_scale: float32 [4096], replicated, may hold values from 0.1 to 1.9
- expert_choice_index: int32 [4096, 2], P('ep'), may hold values from 0 to 15, all different within a row; in each aligned block of 512 rows (0 to 511, 512 to 1023, ...) at most 96 rows name the same one
- group_likelihood: float32 [4096], P('ep'), may hold values from 0.2 to 1
- expert_raw_weight: float32 [4096, 2], P('ep'), may hold values from 0.1 to 1
- gate_weight: bfloat16 [16, 4096, 1024], P('ep', None, 'tp'), may hold values from -0.09375 to 0.09375
- up_weight: bfloat16 [16, 4096, 1024], P('ep', None, 'tp'), may hold values from -0.09375 to 0.09375
- down_weight: bfloat16 [16, 1024, 4096], P('ep', 'tp'), may hold values from -0.1875 to 0.1875
Outputs:
- mixed: bfloat16 [8192, 4096], P(('ep', 'tp'))
- routed: bfloat16 [4096, 4096], P('ep', 'tp')
The draws below stay inside these ranges and needn't reach their ends.
Inputs may be any that keep to these rules, and one draw needn't show every extreme that they name: `expert_choice_index`: each row names 2 different experts. Within the 512 rows of one index of ep (aligned blocks) no expert is named more than 96 times, and in some blocks one expert is named exactly 96 times.
All inputs are finite; a program needn't handle non-finite values.
Results may differ from the reference program's by a relative error of at most 0.012.
Values may be sent and summed in bfloat16 or wider, within the bound.
A program may use at most 192 MiB of HBM per device.

```python
import math
import jax
import jax.numpy as jnp
import numpy as np
from jax import lax

D = 4096
HEADS = 8
QK = 128
VH = 256
FFE = 1024
TOPK = 2
BLOCK = 128
TA_DEV = 1024
TB_DEV = 512
EXPERTS = 16
TOKA = 8192
TOKB = 4096
CAP = 96
N_EP = 8
N_TP = 4


def draw_log_input_gate(key, part):
    key_one = jax.random.fold_in(key, 0)
    base = -1.5 + 1.5 * jax.random.truncated_normal(key_one, -3.0, 3.0, (TOKA, HEADS), jnp.float32)
    return base


def draw_forget_preactivation(key, part):
    key_one, key_two, key_three, key_four, key_five = jax.random.split(key, 5)
    slow_heads = jax.random.uniform(key_one, (HEADS,), jnp.float32) < 0.5
    jitter = 0.6 * jax.random.truncated_normal(key_four, -2.0, 2.0, (TOKA, HEADS), jnp.float32)
    slow_rate = 0.5 / TOKA * jnp.exp(jax.random.uniform(key_two, (HEADS,), jnp.float32, -0.5, 0.5))
    fast_rate = jnp.exp(jax.random.uniform(key_three, (HEADS,), jnp.float32, math.log(1.0 / 50.0), math.log(1.0 / 30.0)))
    head_rate = jnp.where(slow_heads, slow_rate, fast_rate)
    device_factor = jnp.exp(jax.random.uniform(key_five, (TOKA // TA_DEV, HEADS), jnp.float32, -math.log(2.0), math.log(2.0)))
    device_factor = jnp.repeat(device_factor, TA_DEV, axis=0)
    rate = head_rate[None, :] * device_factor * jnp.exp(jitter)
    return -jnp.log(jnp.expm1(rate))


def draw_forget_offset(key, part):
    key_one, key_two = jax.random.split(key, 2)
    spots = jax.random.randint(key_one, (4,), 0, TOKA)
    struck = jnp.any(jnp.arange(TOKA, dtype=jnp.int32)[:, None] == spots[None, :], axis=1)
    depth = jnp.log(jax.random.uniform(key_two, (TOKA, HEADS), jnp.float32, 0.5, 0.8))
    return jnp.where(struck[:, None], depth, 0.0)


def steps_of(stream_key, extent, shards, least, high):
    def one(dim, blocks):
        draws = jax.random.uniform(jax.random.fold_in(jax.random.fold_in(stream_key, 6), dim), (blocks,), jnp.float32, least / len(shards), high / len(shards))
        return jnp.repeat(jnp.exp(draws), extent[dim] // blocks).reshape((-1,) + (1,) * (len(extent) - dim - 1))

    gain = one(*shards[0])
    for cut in shards[1:]:
        gain = gain * one(*cut)
    return gain


def routed_block(rng, own, number, rows, count, top, most, lean):
    order = jax.random.permutation(rng, count)
    packed, ordinary = portions_of(count, rows * top, most, lean, True), portions_of(count, rows * top, most, lean, False)
    places = jnp.arange(count)

    def named(lengths, turn):
        used = int((lengths > 0).sum())
        fixed = max(1, used // 4)
        shifted = fixed + (places - fixed + turn * (used - fixed)) % max(1, count - fixed)
        return jnp.zeros((count,), jnp.int32).at[order[jnp.where(places < fixed, places, shifted)]].set(jnp.asarray(lengths, jnp.int32))

    lengths = jnp.where(number % 4 == 0, named(packed, number // 4), named(ordinary, number - number // 4 - 1))
    mixed = jax.random.permutation(jax.random.fold_in(own, 3), count)
    donor, sink = mixed[0:count // 2 * 2:2], mixed[1:count // 2 * 2:2]
    margin = jnp.minimum(lengths[donor] - 1, most - lengths[sink]) // 2
    margin = jnp.where((donor == order[0]) | (sink == order[0]) | (lengths[sink] == 0), 0, jnp.maximum(margin, 0))
    shifted = jax.random.randint(jax.random.fold_in(own, 4), (count // 2,), 0, 1 << 20) % (margin + 1)
    lengths = lengths.at[donor].add(-shifted).at[sink].add(shifted)
    members = jnp.searchsorted(jnp.cumsum(lengths), jnp.arange(rows * top), side="right").astype(jnp.int32)
    grid = members.reshape(top, rows).T
    grid = grid[jax.random.permutation(jax.random.fold_in(own, 1), rows)]
    turn = jax.random.randint(jax.random.fold_in(own, 2), (rows, 1), 0, top)
    return jnp.take_along_axis(grid, (jnp.arange(top)[None, :] + turn) % top, axis=1)


def portions_of(count, total, reach, lean, full):
    loads = [(1 << 20) // math.isqrt(standing ** lean) + 1 for standing in range(1, count + 1)]
    largest = reach if full else min(reach, max(-(-total // count), total * loads[0] // sum(loads)))
    least = 1 if total - largest >= count - 1 else 0
    holding, rest = [largest] + [least] * (count - 1), total - largest - least * (count - 1)
    while rest > 0:
        candidates = [i for i in range(1, count) if holding[i] < largest] or [i for i in range(1, count) if holding[i] < reach]
        whole, left = sum([loads[i] for i in candidates]), rest
        for i in candidates:
            extra = min(reach - holding[i], max(1, left * loads[i] // whole), rest)
            holding[i] = holding[i] + extra
            rest = rest - extra
    return np.array(holding)


def noise(own_key, shape, deviation, limit, cuts=(), held_as=jnp.bfloat16):
    entries = deviation * jax.random.normal(own_key, shape, jnp.float32)
    if cuts:
        entries = entries * steps_of(own_key, shape, cuts, -0.22, 0.18)
    return jnp.clip(entries, -limit, limit).astype(held_as)


def setup_inputs(seed: int = 0) -> dict:
    streams_of = jax.random.split(jax.random.key(seed), 17)
    queries = noise(streams_of[0], (TOKA, HEADS * QK), 1.0, 6.0, ((0, 8), (1, 4)))
    keys = noise(streams_of[1], (TOKA, HEADS * QK), 1.0, 6.0, ((0, 8), (1, 4)))
    values = noise(streams_of[2], (TOKA, HEADS * VH), 1.0, 6.0, ((0, 8), (1, 4)))
    log_input_gate = draw_log_input_gate(jax.random.fold_in(streams_of[16], 71), 0)
    forget_preactivation = draw_forget_preactivation(jax.random.fold_in(streams_of[16], 71), 0)
    forget_offset = draw_forget_offset(jax.random.fold_in(streams_of[16], 71), 0)
    head_norm_scale = jnp.clip(1.0 + 0.18 * jax.random.normal(streams_of[6], (HEADS * VH,), jnp.float32), 0.1, 1.9)
    memory_output_weight = noise(streams_of[7], (HEADS * VH, D), (HEADS * VH) ** -0.5, 0.125, ((0, 4),))
    second_micro_tokens = noise(streams_of[8], (TOKB, D), 1.0, 6.0, ((0, 8),))
    expert_norm_scale = jnp.clip(1.0 + 0.18 * jax.random.normal(streams_of[9], (D,), jnp.float32), 0.1, 1.9)
    expert_choice_index_keys = jax.random.split(jax.random.fold_in(streams_of[10], 1), TOKB // TB_DEV)
    expert_choice_index_turns = jax.random.permutation(jax.random.fold_in(streams_of[10], 3), TOKB // TB_DEV)
    expert_choice_index = jax.vmap(lambda own, number: routed_block(jax.random.fold_in(streams_of[10], 2), own, number, TB_DEV, EXPERTS, TOPK, CAP, 1))(expert_choice_index_keys, expert_choice_index_turns).reshape((TOKB, TOPK))
    group_likelihood = jnp.clip(0.2 + 0.8 * jax.random.uniform(streams_of[11], (TOKB,), jnp.float32) ** steps_of(streams_of[11], (TOKB,), ((0, 8),), -0.2, 0.2), 0.2, 1.0)
    expert_raw_weight = jnp.clip(jnp.exp(math.log(1.0) - 2.3025851 * jax.random.uniform(streams_of[12], (TOKB, TOPK), jnp.float32) ** steps_of(streams_of[12], (TOKB, TOPK), ((0, 8),), -0.2, 0.2)), 0.1, 1.0)
    gate_weight = noise(streams_of[13], (EXPERTS, D, FFE), D ** -0.5, 0.09375, ((0, 8), (2, 4)))
    up_weight = noise(streams_of[14], (EXPERTS, D, FFE), D ** -0.5, 0.09375, ((0, 8), (2, 4)))
    down_weight = noise(streams_of[15], (EXPERTS, FFE, D), FFE ** -0.5, 0.1875, ((0, 8), (1, 4)))
    return dict(queries=queries, keys=keys, values=values, log_input_gate=log_input_gate, forget_preactivation=forget_preactivation, forget_offset=forget_offset, head_norm_scale=head_norm_scale, memory_output_weight=memory_output_weight, second_micro_tokens=second_micro_tokens, expert_norm_scale=expert_norm_scale, expert_choice_index=expert_choice_index, group_likelihood=group_likelihood, expert_raw_weight=expert_raw_weight, gate_weight=gate_weight, up_weight=up_weight, down_weight=down_weight)


EPSILON = 1e-06
FLOOR_LOG = -1e+30
HIGHEST = lax.Precision.HIGHEST

def memory_block(carry, piece):
    memory, stable_old = carry
    query_block, key_block, value_block, in_gate, forget_log_factor = piece
    query_float = query_block.astype(jnp.float32)
    key_float = key_block.astype(jnp.float32)
    value_float = value_block.astype(jnp.float32)
    qk_scale = 1.0 / math.sqrt(QK)
    raw_scores = jnp.einsum('htd,hsd->hts', query_float, key_float, precision=HIGHEST) * qk_scale
    running = jnp.cumsum(forget_log_factor, axis=-1)
    totals = running[:, -1]
    causal = jnp.tril(jnp.ones((BLOCK, BLOCK), dtype=bool))
    log_weight = jnp.where(causal, running[:, :, None] - running[:, None, :] + in_gate[:, None, :], -jnp.inf)
    carried = running + stable_old[:, None]
    stable = jnp.maximum(carried, lax.optimization_barrier(jnp.max(log_weight, axis=-1)))
    inner = (raw_scores * jnp.exp(log_weight - stable[..., None])).astype(jnp.bfloat16)
    inner = lax.optimization_barrier(inner).astype(jnp.float32)
    outer = jnp.exp(carried - stable)
    memory_half = lax.optimization_barrier(memory.astype(jnp.bfloat16)).astype(jnp.float32)
    state = outer[..., None] * jnp.einsum('htd,hde->hte', query_float, memory_half, precision=HIGHEST)
    state = state + jnp.einsum('hts,hse->hte', inner, value_float, precision=HIGHEST)
    to_end = totals[:, None] - running + in_gate
    block_peak = lax.optimization_barrier(jnp.max(to_end, axis=-1))
    scaled_keys = key_float * qk_scale
    weighted = (scaled_keys * jnp.exp(to_end - block_peak[:, None])[..., None]).astype(jnp.bfloat16)
    weighted = lax.optimization_barrier(weighted).astype(jnp.float32)
    update = jnp.einsum('hsd,hse->hde', weighted, value_float, precision=HIGHEST)
    stable_new = jnp.maximum(totals + stable_old, block_peak)
    memory = jnp.exp(totals + stable_old - stable_new)[:, None, None] * memory + jnp.exp(block_peak - stable_new)[:, None, None] * update
    return ((memory, stable_new), state)

def recurrence_baseline(queries, keys, values, log_input_gate, forget_preactivation, forget_offset, head_norm_scale, memory_output_weight):
    block_count = TOKA // BLOCK

    def to_blocks(array, width):
        return array.reshape(block_count, BLOCK, HEADS, width).transpose(0, 2, 1, 3)
    forget_log_factor = jax.nn.log_sigmoid(forget_preactivation) + forget_offset
    gate_blocks = log_input_gate.reshape(block_count, BLOCK, HEADS).transpose(0, 2, 1)
    forget_blocks = forget_log_factor.reshape(block_count, BLOCK, HEADS).transpose(0, 2, 1)
    start = (jnp.zeros((HEADS, QK, VH), jnp.float32), jnp.full((HEADS,), FLOOR_LOG, jnp.float32))
    unused, states = lax.scan(memory_block, start, (to_blocks(queries, QK), to_blocks(keys, QK), to_blocks(values, VH), gate_blocks, forget_blocks))
    states = states * lax.rsqrt(lax.optimization_barrier(jnp.mean(states * states, axis=-1, keepdims=True)) + EPSILON)
    hidden = states.transpose(0, 2, 1, 3).reshape(TOKA, HEADS * VH)
    hidden = (hidden * head_norm_scale).astype(jnp.bfloat16)
    group_width = HEADS // N_TP * VH
    total = jnp.zeros((TOKA, D), jnp.float32)
    for group in range(N_TP):
        part = jnp.dot(hidden[:, group * group_width:(group + 1) * group_width], memory_output_weight[group * group_width:(group + 1) * group_width], preferred_element_type=jnp.float32).astype(jnp.bfloat16)
        part = lax.optimization_barrier(part)
        total = total + part.astype(jnp.float32)
    return total.astype(jnp.bfloat16)

def expert_reference(second_micro_tokens, expert_norm_scale, expert_choice_index, group_likelihood, expert_raw_weight, gate_weight, up_weight, down_weight):
    token_float = second_micro_tokens.astype(jnp.float32)
    normed = token_float * lax.rsqrt(lax.optimization_barrier(jnp.mean(token_float * token_float, axis=-1, keepdims=True)) + EPSILON)
    normed = (normed * expert_norm_scale).astype(jnp.bfloat16)
    share = expert_raw_weight / lax.optimization_barrier(jnp.sum(expert_raw_weight, axis=1, keepdims=True))
    route_weight = group_likelihood[:, None] * share
    slot_limit = N_EP * CAP
    unit_width = FFE // N_TP

    def one_expert(total, expert):
        chosen = expert_choice_index == expert
        row_hit = jnp.any(chosen, axis=1)
        row_weight = lax.optimization_barrier(jnp.sum(jnp.where(chosen, route_weight, 0.0), axis=1))
        picked = jnp.nonzero(row_hit, size=slot_limit, fill_value=0)[0].astype(jnp.int32)
        live = (jnp.arange(slot_limit, dtype=jnp.int32) < jnp.sum(row_hit.astype(jnp.int32))).astype(jnp.float32)
        gathered = normed[picked]
        gate = jnp.dot(gathered, gate_weight[expert], preferred_element_type=jnp.float32)
        upward = jnp.dot(gathered, up_weight[expert], preferred_element_type=jnp.float32)
        hidden = (jax.nn.silu(gate) * upward).astype(jnp.bfloat16)
        down = down_weight[expert]
        summed = jnp.zeros((slot_limit, D), jnp.float32)
        for group in range(N_TP):
            part = jnp.dot(hidden[:, group * unit_width:(group + 1) * unit_width], down[group * unit_width:(group + 1) * unit_width], preferred_element_type=jnp.float32).astype(jnp.bfloat16)
            part = lax.optimization_barrier(part)
            summed = summed + part.astype(jnp.float32)
        expert_out = lax.optimization_barrier(summed.astype(jnp.bfloat16))
        contrib = expert_out.astype(jnp.float32) * (row_weight[picked] * live)[:, None]
        return (total.at[picked].add(contrib), None)
    total, unused = lax.scan(one_expert, jnp.zeros((TOKB, D), jnp.float32), jnp.arange(EXPERTS, dtype=jnp.int32))
    return total.astype(jnp.bfloat16)

def reference(queries, keys, values, log_input_gate, forget_preactivation, forget_offset, head_norm_scale, memory_output_weight, second_micro_tokens, expert_norm_scale, expert_choice_index, group_likelihood, expert_raw_weight, gate_weight, up_weight, down_weight):
    mixed = recurrence_baseline(queries, keys, values, log_input_gate, forget_preactivation, forget_offset, head_norm_scale, memory_output_weight)
    routed = expert_reference(second_micro_tokens, expert_norm_scale, expert_choice_index, group_likelihood, expert_raw_weight, gate_weight, up_weight, down_weight)
    return (mixed, routed)
```

```python
import functools
import math

import jax
import jax.numpy as jnp
from jax import lax
from jax.experimental import pallas as pl
from jax.experimental.pallas import tpu as pltpu
from jax.sharding import PartitionSpec as P

BLOCK = 128
EPSILON = 1e-06
FLOOR_LOG = -1e30
LANES = 128
MESH = pl.DeviceIdType.MESH
F32 = jnp.float32
BF16 = jnp.bfloat16


def flip(index, mask):
    bit = 1
    while bit <= mask:
        if mask & bit:
            index = index + bit * (1 - 2 * ((index // bit) % 2))
        bit *= 2
    return index


def dot(left, right, dims=((1,), (0,))):
    return lax.dot_general(left, right, (dims, ((), ())), preferred_element_type=F32)


def kernel(
    n,
    tp,
    a_ref,
    b_ref,
    q_hbm,
    k_hbm,
    v_hbm,
    cols_ref,
    arow_ref,
    gp_ref,
    hscale_ref,
    wo_hbm,
    gate_hbm,
    up_hbm,
    down_hbm,
    mixed_ref,
    ret_ref,
    rows,
    gw,
    uw,
    dcols,
    fh,
    res,
    part,
    crecv,
    xrecv,
    qb,
    kb,
    vb,
    hid,
    wo,
    cst,
    cin,
    tabs,
    stat,
    stats,
    st_send,
    st_buf,
    low_send,
    low_buf,
    load_sem,
    a_send,
    a_recv,
    b_send,
    b_recv,
    f_send,
    f_recv,
    h_send,
    h_recv,
    w_send,
    w_recv,
    s_send,
    s_recv,
    t_send,
    t_recv,
    l_send,
    l_recv,
    m_send,
    m_recv,
    r_send,
    r_recv,
):
    me, t = lax.axis_index("ep"), lax.axis_index("tp")
    half = n // 2
    group_count = 4
    per_group = n // group_count
    local_experts, cap, width = a_ref.shape[1:]
    units = gw.shape[2]
    block_count, head_count = cst.shape[0] - 1, cst.shape[1]
    key_width, value_width = cst.shape[2:]
    row_count = qb.shape[0]
    part_rows = part.shape[1]
    model = rows.shape[2]
    t1, t2 = flip(t, 1), flip(t, 2)
    core, side = t % 2, t // 2
    base = (me // half) * half
    slot = me - base

    def peer(mask):
        return {"ep": flip(me, mask)}

    def window(index):
        return pl.ds(pl.multiple_of(index * width, LANES), width)

    def unit_window(index):
        return pl.ds(pl.multiple_of(index * units, LANES), units)

    def remote(src, dst, send, recv, device):
        return pltpu.make_async_remote_copy(
            src_ref=src,
            dst_ref=dst,
            send_sem=send,
            recv_sem=recv,
            device_id=device,
            device_id_type=MESH,
        )

    barrier = pltpu.get_barrier_semaphore()
    for mask in range(1, n):
        pl.semaphore_signal(barrier, inc=1, device_id=peer(mask), device_id_type=MESH)
    for mask in range(1, tp):
        pl.semaphore_signal(
            barrier, inc=1, device_id={"tp": flip(t, mask)}, device_id_type=MESH
        )

    loads = {}

    def load(name, src, dst):
        loads[name] = pltpu.make_async_copy(src, dst, load_sem.at[len(loads)])
        loads[name].start()

    load("k", k_hbm, kb)
    load("v", v_hbm, vb)
    load("q", q_hbm, qb)
    load("a0", a_ref.at[0], rows.at[:, pl.ds(0, cap), window(t)])
    load("b0", b_ref.at[0], rows.at[:, pl.ds(0, cap), window(t2)])
    load("wo", wo_hbm, wo)
    load("gate", gate_hbm, gw)
    load("up", up_hbm, uw)
    load("down", down_hbm.at[:, :, window(t)], dcols.at[:, unit_window(t), :])
    pl.semaphore_wait(barrier, n - 1 + tp - 1)

    sends = []

    def start(copy):
        copy.start()
        sends.append(copy)
        return copy

    def slots(mask, count=1):
        return pl.ds(mask * cap, count * cap)

    a_copy, b_copy = {}, {}

    def dispatch(mask):
        a_copy[mask] = start(
            remote(
                a_ref.at[mask],
                rows.at[:, slots(mask), window(t)],
                a_send.at[mask],
                a_recv.at[mask],
                peer(mask),
            )
        )
        if mask < half:
            b_copy[mask] = start(
                remote(
                    b_ref.at[mask],
                    rows.at[:, slots(mask), window(t2)],
                    b_send.at[mask],
                    b_recv.at[mask],
                    peer(mask),
                )
            )

    def forward_x(mask):
        a_copy[mask].wait_recv()
        view = rows.at[:, slots(mask), window(t)]
        b_copy[mask] = start(
            remote(view, view, b_send.at[mask], b_recv.at[mask], {"tp": t2})
        )

    group_masks = [range(g * per_group, (g + 1) * per_group) for g in range(group_count)]
    near_groups = [g for g in range(group_count) if group_masks[g][0] < half]
    dispatch(group_masks[2][0])
    w_copy = {}
    for mask in (2, 3, 1):
        w_copy[mask] = start(
            remote(
                down_hbm.at[:, :, window(flip(t, mask))],
                dcols.at[:, unit_window(t), :],
                w_send.at[mask],
                w_recv.at[mask],
                {"tp": flip(t, mask)},
            )
        )
    for mask in group_masks[0]:
        if mask:
            dispatch(mask)

    TQ, TC, TW1, TW2, TF, TWI, TWL = range(7)
    stable = jnp.full((1, LANES), FLOOR_LOG, F32)
    total = jnp.zeros((1, LANES), F32)
    for b in range(block_count):
        span, peak = gp_ref[0, b : b + 1, :], gp_ref[1, b : b + 1, :]
        tabs[TQ, b : b + 1, :] = total
        tabs[TC, b : b + 1, :] = stable
        newer = jnp.maximum(span + stable, peak)
        tabs[TW1, b : b + 1, :] = jnp.exp(span + stable - newer)
        tabs[TW2, b : b + 1, :] = jnp.exp(peak - newer)
        stable, total = newer, total + span
    stat[0:1, :] = stable
    stat[1:2, :] = total
    stats[me, 0:1, :] = stable
    stats[me, 1:2, :] = total

    loads["k"].wait()
    loads["v"].wait()
    cst[0] = jnp.zeros(cst.shape[1:], F32)

    def gather_block(b, carry):
        at = pl.ds(pl.multiple_of(b * BLOCK, BLOCK), BLOCK)
        for h in range(head_count):
            keyed = kb[at, h * key_width : (h + 1) * key_width].astype(F32)
            weight = cols_ref[at, head_count + h : head_count + h + 1]
            update = dot(
                (keyed * weight).astype(BF16),
                vb[at, h * value_width : (h + 1) * value_width],
                ((0,), (0,)),
            )
            old = tabs[TW1, pl.ds(b, 1), h : h + 1]
            new = tabs[TW2, pl.ds(b, 1), h : h + 1]
            cst[b + 1, h] = old * cst[b, h] + new * update
        return carry

    lax.fori_loop(0, block_count, gather_block, 0)
    st_send[...] = cst[block_count].astype(BF16)
    st_buf[slot] = cst[block_count].astype(BF16)
    s_copy = {
        mask: start(
            remote(stat, stats.at[me], s_send.at[mask], s_recv.at[mask], peer(mask))
        )
        for mask in range(1, n)
    }
    t_copy = {
        mask: start(
            remote(st_send, st_buf.at[slot], t_send.at[mask], t_recv.at[mask], peer(mask))
        )
        for mask in range(1, half)
    }
    for mask in group_masks[2][1:]:
        dispatch(mask)
    for mask in group_masks[1][: per_group // 2]:
        dispatch(mask)

    for mask in range(1, n):
        s_copy[mask].wait_recv()
    for mask in range(1, half):
        t_copy[mask].wait_recv()

    low_log, suffix = [None] * half, jnp.zeros((1, LANES), F32)
    for j in reversed(range(half)):
        low_log[j] = stats[j, 0:1, :] + suffix
        suffix = suffix + stats[j, 1:2, :]
    low_stable = functools.reduce(jnp.maximum, low_log)
    low_weight = [jnp.exp(value - low_stable) for value in low_log]

    l_copy = remote(
        low_send, low_buf, l_send.at[0], l_recv.at[0], {"ep": flip(me, half)}
    )

    @pl.when(me < half)
    def _():
        for h in range(head_count):
            summed = jnp.zeros((key_width, value_width), F32)
            for j in range(half):
                summed = summed + low_weight[j][:, h : h + 1] * st_buf[j, h].astype(F32)
            low_send[h] = summed.astype(BF16)
        low_buf[...] = jnp.zeros(low_buf.shape, BF16)
        l_copy.start()

    for mask in group_masks[3]:
        dispatch(mask)
    for mask in group_masks[1][per_group // 2 :]:
        dispatch(mask)

    for mask in group_masks[2]:
        forward_x(mask)

    logs, valid, suffix = [None] * half, [None] * half, jnp.zeros((1, LANES), F32)
    for j in reversed(range(half)):
        valid[j] = j < slot
        logs[j] = jnp.where(valid[j], stats[base + j, 0:1, :] + suffix, FLOOR_LOG)
        suffix = jnp.where(valid[j], suffix + stats[base + j, 1:2, :], suffix)
    low_in = jnp.where(me >= half, low_stable + suffix, FLOOR_LOG)
    peak_in = functools.reduce(jnp.maximum, logs + [low_in])
    weights = [
        jnp.where(valid[j], jnp.exp(logs[j] - peak_in), 0.0) for j in range(half)
    ]
    low_in = jnp.where(me >= half, jnp.exp(low_in - peak_in), 0.0)
    carried_stable = tabs[TQ] + peak_in
    full_stable = jnp.maximum(carried_stable, tabs[TC])
    tabs[TF] = full_stable
    tabs[TWI] = jnp.exp(carried_stable - full_stable)
    tabs[TWL] = jnp.exp(tabs[TC] - full_stable)

    @pl.when(me >= half)
    def _():
        l_copy.wait_recv()

    for h in range(head_count):
        summed = low_in[:, h : h + 1] * low_buf[h].astype(F32)
        for j in range(half):
            summed = summed + weights[j][:, h : h + 1] * st_buf[j, h].astype(F32)
        cin[h] = summed

    loads["q"].wait()
    scale = 1.0 / math.sqrt(key_width)
    causal = lax.broadcasted_iota(jnp.int32, (BLOCK, BLOCK), 0) >= lax.broadcasted_iota(
        jnp.int32, (BLOCK, BLOCK), 1
    )

    def read_block(b, carry):
        at = pl.ds(pl.multiple_of(b * BLOCK, BLOCK), BLOCK)
        for h in range(head_count):
            query = qb[at, h * key_width : (h + 1) * key_width]
            key = kb[at, h * key_width : (h + 1) * key_width]
            value = vb[at, h * value_width : (h + 1) * value_width]
            running = cols_ref[at, h : h + 1]
            other = arow_ref[pl.ds(h * block_count + b, 1), :]
            scores = dot(query, key, ((1,), (1,))) * scale
            log_weight = jnp.where(causal, running + other, FLOOR_LOG)
            carried = running + tabs[TF, pl.ds(b, 1), h : h + 1]
            highest = jnp.maximum(carried, jnp.max(log_weight, axis=1, keepdims=True))
            inner = (scores * jnp.exp(log_weight - highest)).astype(BF16)
            memory = (
                tabs[TWI, pl.ds(b, 1), h : h + 1] * cin[h]
                + tabs[TWL, pl.ds(b, 1), h : h + 1] * cst[b, h]
            ).astype(BF16)
            state = jnp.exp(carried - highest) * dot(query, memory) + dot(inner, value)
            mean = jnp.mean(state * state, axis=1, keepdims=True)
            state = state * lax.rsqrt(mean + EPSILON)
            at_head = slice(h * value_width, (h + 1) * value_width)
            hid[at, at_head] = (state * hscale_ref[:, at_head]).astype(BF16)
        return carry

    lax.fori_loop(0, block_count, read_block, 0)

    loads["wo"].wait()
    tile = 256

    def project(index):
        left = hid[pl.ds(pl.multiple_of(index * part_rows, part_rows), part_rows), :]

        def piece(i, carry):
            at = pl.ds(pl.multiple_of(i * tile, tile), tile)
            part[index, :, at] = dot(left, wo[:, at]).astype(BF16)
            return carry

        lax.fori_loop(0, model // tile, piece, 0)

    m_copy = []
    for i in range(2):
        project(2 * i + 1 - core)
        m_copy.append(
            start(
                remote(
                    part.at[2 * i + 1 - core],
                    crecv.at[i],
                    m_send.at[i],
                    m_recv.at[i],
                    {"tp": t1},
                )
            )
        )
    project(t2)
    for copy in m_copy:
        copy.wait_recv()
    chunk = 32

    def add_other(i, carry):
        at = pl.ds(pl.multiple_of(i * chunk, chunk), chunk)
        part[t2, at, :] = (
            part[t2, at, :].astype(F32) + crecv[1 - side, at, :].astype(F32)
        ).astype(BF16)
        return carry

    lax.fori_loop(0, part_rows // chunk, add_other, 0)

    f_copy, h_copy = {}, {}

    def stage_core(g, which):
        if which == 0:
            for mask in group_masks[g]:
                if mask == 0:
                    loads["a0"].wait()
                elif mask < half:
                    a_copy[mask].wait_recv()
        else:
            for mask in group_masks[g]:
                if mask == 0:
                    loads["b0"].wait()
                else:
                    b_copy[mask].wait_recv()
        view = rows.at[
            :, slots(group_masks[g][0], per_group), window(t if which == 0 else t2)
        ]
        f_copy[g, which] = start(
            remote(view, view, f_send.at[which, g], f_recv.at[which, g], {"tp": t1})
        )

    def group_slots(g):
        return slots(group_masks[g][0], per_group)

    def send_units(g, kind, owner, target):
        view = fh.at[:, group_slots(g), unit_window(owner)]
        h_copy[g, kind] = start(
            remote(view, view, h_send.at[kind, g], h_recv.at[kind, g], {"tp": target})
        )

    weights_ready = []

    def stage_hidden(g):
        f_copy[g, 0].wait_recv()
        f_copy[g, 1].wait_recv()
        if not weights_ready:
            loads["gate"].wait()
            loads["up"].wait()
            weights_ready.append(True)

        def one(e, carry):
            left = rows[e, group_slots(g), :]
            gate = dot(left, gw[e])
            upward = dot(left, uw[e])
            fh[e, group_slots(g), unit_window(t)] = (
                gate * jax.nn.sigmoid(gate) * upward
            ).astype(BF16)
            return carry

        lax.fori_loop(0, local_experts, one, 0)
        send_units(g, 0, t, t2)
        send_units(g, 1, t, t1)

    def stage_units(g):
        h_copy[g, 0].wait_recv()
        send_units(g, 2, t2, t1)

    down_ready = []
    r_copy = {}

    def stage_down(g):
        h_copy[g, 1].wait_recv()
        h_copy[g, 2].wait_recv()
        if not down_ready:
            loads["down"].wait()
            for mask in (1, 2, 3):
                w_copy[mask].wait_recv()
            down_ready.append(True)

        def one(i, carry):
            e, c = i // (width // tile), i % (width // tile)
            at = pl.ds(pl.multiple_of(c * tile, tile), tile)
            res[e, group_slots(g), at] = dot(
                fh[e, group_slots(g), :], dcols[e, :, at]
            ).astype(BF16)
            return carry

        lax.fori_loop(0, local_experts * (width // tile), one, 0)
        for mask in group_masks[g]:
            view = res.at[:, slots(mask), :]
            if mask:
                r_copy[mask] = start(
                    remote(
                        view, ret_ref.at[mask], r_send.at[mask], r_recv.at[mask], peer(mask)
                    )
                )
            else:
                load("ret", view, ret_ref.at[0])

    stage_core(2, 0)
    stage_core(2, 1)
    x_copy = start(
        remote(part.at[t2], xrecv, m_send.at[2], m_recv.at[2], {"tp": t2})
    )
    stage_core(0, 0)
    stage_core(0, 1)
    project(t)
    stage_hidden(2)
    stage_hidden(0)
    stage_units(2)
    for mask in group_masks[3]:
        forward_x(mask)
    stage_core(3, 0)
    stage_units(0)
    stage_down(2)
    stage_core(3, 1)
    stage_core(1, 0)
    stage_core(1, 1)
    stage_down(0)
    stage_hidden(3)
    stage_hidden(1)
    stage_units(3)
    stage_units(1)
    stage_down(3)
    stage_down(1)

    x_copy.wait_recv()

    def add_own(i, carry):
        at = pl.ds(pl.multiple_of(i * chunk, chunk), chunk)
        mixed_ref[at, :] = (
            part[t, at, :].astype(F32)
            + crecv[side, at, :].astype(F32)
            + xrecv[at, :].astype(F32)
        ).astype(BF16)
        return carry

    lax.fori_loop(0, part_rows // chunk, add_own, 0)

    loads["ret"].wait()
    for mask in range(1, n):
        r_copy[mask].wait_recv()
    for copy in sends:
        copy.wait_send()

    @pl.when(me < half)
    def _():
        l_copy.wait_send()


def gates(log_input_gate, forget_preactivation, forget_offset, key_width):
    row_count, head_count = log_input_gate.shape
    block_count = row_count // BLOCK
    forget_log = jax.nn.log_sigmoid(forget_preactivation) + forget_offset
    forget_log = forget_log.reshape(block_count, BLOCK, head_count)
    in_gate = log_input_gate.reshape(block_count, BLOCK, head_count)
    lower = jnp.tril(jnp.ones((BLOCK, BLOCK), F32))
    running = jnp.einsum(
        "ts,bsh->bth",
        lower,
        forget_log,
        preferred_element_type=F32,
        precision=lax.Precision.HIGHEST,
    )
    totals = running[:, -1]
    to_end = totals[:, None] - running + in_gate
    peak = jnp.max(to_end, axis=1)
    key_weight = jnp.exp(to_end - peak[:, None]) * (1.0 / math.sqrt(key_width))
    cols = jnp.concatenate([running, key_weight], axis=2).reshape(row_count, -1)
    arow = (in_gate - running).transpose(2, 0, 1).reshape(head_count * block_count, BLOCK)
    gp = jnp.pad(jnp.stack([totals, peak]), ((0, 0), (0, 0), (0, LANES - head_count)))
    return cols, arow, gp


def per_device(
    queries,
    keys,
    values,
    log_input_gate,
    forget_preactivation,
    forget_offset,
    head_norm_scale,
    memory_output_weight,
    second_micro_tokens,
    expert_norm_scale,
    expert_choice_index,
    group_likelihood,
    expert_raw_weight,
    gate_weight,
    up_weight,
    down_weight,
):
    token_count, model_width = second_micro_tokens.shape
    pick_count = expert_choice_index.shape[1]
    local_experts, _, units = gate_weight.shape
    n, tp = lax.axis_size("ep"), lax.axis_size("tp")
    me, t = lax.axis_index("ep"), lax.axis_index("tp")
    half = n // 2
    expert_count = local_experts * n
    cap = tp * max(1, 3 * pick_count * token_count // (2 * expert_count * tp))
    width = model_width // tp
    row_count, head_count = log_input_gate.shape
    key_width = queries.shape[1] // head_count
    value_width = values.shape[1] // head_count
    block_count = row_count // BLOCK
    out_depth = head_count * value_width

    share = expert_raw_weight / jnp.sum(expert_raw_weight, axis=1, keepdims=True)
    route_weight = group_likelihood[:, None] * share

    experts = jnp.arange(expert_count, dtype=jnp.int32)
    named = expert_choice_index[:, :, None] == experts
    named_token = jnp.sum(named.astype(F32), axis=1)
    earlier = jnp.tril(jnp.ones((token_count, token_count), BF16), -1)
    before = jnp.dot(earlier, named_token.astype(BF16), preferred_element_type=F32)
    slot_rank = jnp.sum(jnp.where(named, before[:, None, :], 0.0), axis=2).astype(jnp.int32)
    slot_index = expert_choice_index * cap + slot_rank

    send_shape = (n, local_experts, cap)
    step, expert, row = (lax.broadcasted_iota(jnp.int32, send_shape, i) for i in range(3))
    send_slot = (((me ^ step) * local_experts + expert) * cap + row).reshape(-1)

    token_float = second_micro_tokens.astype(F32)
    inverse = lax.rsqrt(jnp.mean(token_float * token_float, axis=-1, keepdims=True) + EPSILON)

    def normed(index):
        tokens = lax.dynamic_slice_in_dim(second_micro_tokens, index * width, width, 1)
        gain = lax.dynamic_slice_in_dim(expert_norm_scale, index * width, width, 0)
        return (tokens.astype(F32) * inverse * gain).astype(BF16)

    chosen = send_slot[:, None] == slot_index[:, 0][None, :]
    for pick in range(1, pick_count):
        chosen = chosen | (send_slot[:, None] == slot_index[:, pick][None, :])
    chosen = chosen.astype(BF16)
    near = half * local_experts * cap
    out_a = jnp.dot(chosen, normed(t), preferred_element_type=F32).astype(BF16)
    out_b = jnp.dot(chosen[:near], normed(t ^ 2), preferred_element_type=F32).astype(BF16)
    out_a = out_a.reshape(n, local_experts, cap, width)
    out_b = out_b.reshape(half, local_experts, cap, width)

    cols, arow, gp = gates(log_input_gate, forget_preactivation, forget_offset, key_width)

    slot_rows = n * cap
    part_rows = row_count // tp
    vmem = pl.BlockSpec(memory_space=pltpu.VMEM)
    hbm = pl.BlockSpec(memory_space=pl.ANY)
    dma = pltpu.SemaphoreType.DMA
    mixed, returned = pl.pallas_call(
        functools.partial(kernel, n, tp),
        out_shape=(
            jax.ShapeDtypeStruct((part_rows, model_width), BF16),
            jax.ShapeDtypeStruct((n, local_experts, cap, width), BF16),
        ),
        in_specs=[hbm] * 5 + [vmem] * 4 + [hbm] * 4,
        out_specs=(vmem, hbm),
        scratch_shapes=[
            pltpu.VMEM((local_experts, slot_rows, model_width), BF16),
            pltpu.VMEM(gate_weight.shape, BF16),
            pltpu.VMEM(up_weight.shape, BF16),
            pltpu.VMEM((local_experts, tp * units, width), BF16),
            pltpu.VMEM((local_experts, slot_rows, tp * units), BF16),
            pltpu.VMEM((local_experts, slot_rows, width), BF16),
            pltpu.VMEM((tp, part_rows, model_width), BF16),
            pltpu.VMEM((2, part_rows, model_width), BF16),
            pltpu.VMEM((part_rows, model_width), BF16),
            pltpu.VMEM(queries.shape, BF16),
            pltpu.VMEM(keys.shape, BF16),
            pltpu.VMEM(values.shape, BF16),
            pltpu.VMEM((row_count, out_depth), BF16),
            pltpu.VMEM((out_depth, model_width), BF16),
            pltpu.VMEM((block_count + 1, head_count, key_width, value_width), F32),
            pltpu.VMEM((head_count, key_width, value_width), F32),
            pltpu.VMEM((7, block_count, LANES), F32),
            pltpu.VMEM((8, LANES), F32),
            pltpu.VMEM((n, 8, LANES), F32),
            pltpu.VMEM((head_count, key_width, value_width), BF16),
            pltpu.VMEM((half, head_count, key_width, value_width), BF16),
            pltpu.VMEM((head_count, key_width, value_width), BF16),
            pltpu.VMEM((head_count, key_width, value_width), BF16),
            dma((10,)),
            dma((n,)),
            dma((n,)),
            dma((n,)),
            dma((n,)),
            dma((2, 4)),
            dma((2, 4)),
            dma((3, 4)),
            dma((3, 4)),
            dma((tp,)),
            dma((tp,)),
            dma((n,)),
            dma((n,)),
            dma((half,)),
            dma((half,)),
            dma((1,)),
            dma((1,)),
            dma((3,)),
            dma((3,)),
            dma((n,)),
            dma((n,)),
        ],
        compiler_params=pltpu.CompilerParams(
            collective_id=0, has_side_effects=True, vmem_limit_bytes=67043328
        ),
        name="exchange",
    )(
        out_a,
        out_b,
        queries,
        keys,
        values,
        cols,
        arow,
        gp,
        head_norm_scale.reshape(1, -1),
        memory_output_weight,
        gate_weight,
        up_weight,
        down_weight,
    )
    returned = returned.reshape(-1, width)

    spread = jnp.zeros((token_count, send_slot.shape[0]), F32)
    for pick in range(pick_count):
        spread = spread + jnp.where(
            slot_index[:, pick : pick + 1] == send_slot[None, :],
            route_weight[:, pick : pick + 1],
            0.0,
        )
    spread_high = spread.astype(BF16)
    spread_low = (spread - spread_high.astype(F32)).astype(BF16)
    combined = jnp.dot(spread_high, returned, preferred_element_type=F32) + jnp.dot(
        spread_low, returned, preferred_element_type=F32
    )
    return mixed, combined.astype(BF16)


def solution(mesh):
    in_specs = (
        P("ep", "tp"),
        P("ep", "tp"),
        P("ep", "tp"),
        P("ep", "tp"),
        P("ep", "tp"),
        P("ep", "tp"),
        P("tp"),
        P("tp", None),
        P("ep", None),
        P(),
        P("ep", None),
        P("ep"),
        P("ep", None),
        P("ep", None, "tp"),
        P("ep", None, "tp"),
        P("ep", "tp", None),
    )
    out_specs = (P(("ep", "tp"), None), P("ep", "tp"))
    return jax.shard_map(
        per_device, mesh=mesh, in_specs=in_specs, out_specs=out_specs, check_vma=False
    )
```

```python
import functools
import math

import jax
import jax.numpy as jnp
from jax import lax
from jax.experimental import pallas as pl
from jax.experimental.pallas import tpu as pltpu
from jax.sharding import PartitionSpec as P

BLOCK = 128
EPSILON = 1e-06
FLOOR_LOG = -1e30
LANES = 128
MESH = pl.DeviceIdType.MESH
F32 = jnp.float32
BF16 = jnp.bfloat16


def flip(index, mask):
    bit = 1
    while bit <= mask:
        if mask & bit:
            index = index + bit * (1 - 2 * ((index // bit) % 2))
        bit *= 2
    return index


def dot(left, right, dims=((1,), (0,))):
    return lax.dot_general(left, right, (dims, ((), ())), preferred_element_type=F32)


def kernel(
    n,
    tp,
    cap,
    tok_hbm,
    gain_ref,
    choice_ref,
    likelihood_ref,
    raw_ref,
    q_hbm,
    k_hbm,
    v_hbm,
    cols_ref,
    arow_ref,
    gp_ref,
    hscale_ref,
    wo_hbm,
    gate_hbm,
    up_hbm,
    down_hbm,
    xrecv,
    routed_ref,
    rows,
    gw,
    uw,
    dcols,
    fh,
    res,
    part,
    crecv,
    qb,
    kb,
    vb,
    hid,
    wo,
    cst,
    tabs,
    stat,
    stats,
    st_buf,
    low_send,
    low_buf,
    ret,
    other_nb,
    bbuf,
    route_col,
    slot_row,
    load_sem,
    a_send,
    a_recv,
    b_send,
    b_recv,
    f_send,
    f_recv,
    h_send,
    h_recv,
    w_send,
    w_recv,
    s_send,
    s_recv,
    t_send,
    t_recv,
    l_send,
    l_recv,
    m_send,
    m_recv,
    r_send,
    r_recv,
):
    me, t = lax.axis_index("ep"), lax.axis_index("tp")
    half = n // 2
    group_count = 4
    per_group = n // group_count
    local_experts, _, width = res.shape
    token_count = routed_ref.shape[0]
    nb = (routed_ref, other_nb)
    rows_sent = local_experts * cap
    units = gw.shape[2]
    block_count, head_count = cst.shape[0] - 1, cst.shape[1]
    key_width, value_width = cst.shape[2:]
    row_count = qb.shape[0]
    part_rows = part.shape[1]
    model = rows.shape[2]
    t1, t2 = flip(t, 1), flip(t, 2)
    core, side = t % 2, t // 2
    base = (me // half) * half
    slot = me - base

    def peer(mask):
        return {"ep": flip(me, mask)}

    def window(index):
        return pl.ds(pl.multiple_of(index * width, LANES), width)

    def unit_window(index):
        return pl.ds(pl.multiple_of(index * units, LANES), units)

    def remote(src, dst, send, recv, device):
        return pltpu.make_async_remote_copy(
            src_ref=src,
            dst_ref=dst,
            send_sem=send,
            recv_sem=recv,
            device_id=device,
            device_id_type=MESH,
        )

    barrier = pltpu.get_barrier_semaphore()
    for mask in range(1, n):
        pl.semaphore_signal(barrier, inc=1, device_id=peer(mask), device_id_type=MESH)
    for mask in range(1, tp):
        pl.semaphore_signal(
            barrier, inc=1, device_id={"tp": flip(t, mask)}, device_id_type=MESH
        )

    loads = {}

    def load(name, src, dst):
        loads[name] = pltpu.make_async_copy(src, dst, load_sem.at[len(loads)])
        loads[name].start()

    token_tiles = token_count // part_rows
    load("tokens", tok_hbm, part.at[pl.ds(0, token_tiles)])
    load("k", k_hbm, kb)
    load("v", v_hbm, vb)
    load("q", q_hbm, qb)
    load("wo", wo_hbm, wo)
    load("gate", gate_hbm, gw)
    load("up", up_hbm, uw)
    load("down", down_hbm.at[:, :, window(t)], dcols.at[:, unit_window(t), :])
    pl.semaphore_wait(barrier, n - 1 + tp - 1)

    sends, sent = [], set()
    tile, wide = 256, 512

    def start(copy):
        copy.start()
        sends.append(copy)
        return copy

    def slots(mask, count=1):
        return pl.ds(mask * cap, count * cap)

    a_copy, b_copy = {}, {}

    def select(mask, which, store):
        first = flip(me, mask) * rows_sent
        ids = lax.broadcasted_iota(jnp.int32, (rows_sent, token_count), 0) + first
        ids = ids.astype(F32)
        chosen = (slot_row[4:5, :] == ids) | (slot_row[5:6, :] == ids)
        chosen = jnp.where(chosen, 1.0, 0.0).astype(BF16)

        def piece(i, carry):
            at = pl.multiple_of(i * wide, wide)
            picked = dot(chosen, nb[which][:, pl.ds(at, wide)])
            for e in range(local_experts):
                store(e, at, picked[e * cap : (e + 1) * cap].astype(BF16))
            return carry

        lax.fori_loop(0, width // wide, piece, 0)

    def dispatch(mask):
        def store_a(e, at, value):
            res[e, slots(mask), pl.ds(at, wide)] = value

        def store_b(e, at, value):
            bbuf[mask - 1, e, :, pl.ds(at, wide)] = value

        select(mask, 0, store_a)
        a_copy[mask] = start(
            remote(
                res.at[:, slots(mask), :],
                rows.at[:, slots(mask), window(t)],
                a_send.at[mask],
                a_recv.at[mask],
                peer(mask),
            )
        )
        if mask < half:
            select(mask, 1, store_b)
            b_copy[mask] = start(
                remote(
                    bbuf.at[mask - 1],
                    rows.at[:, slots(mask), window(t2)],
                    b_send.at[mask],
                    b_recv.at[mask],
                    peer(mask),
                )
            )

    def keep_own():
        for which, owner in enumerate((t, t2)):

            def store(e, at, value):
                begin = pl.multiple_of(owner * width + at, wide)
                rows[e, slots(0), pl.ds(begin, wide)] = value

            select(0, which, store)

    def forward_x(mask):
        a_copy[mask].wait_recv()
        view = rows.at[:, slots(mask), window(t)]
        b_copy[mask] = start(
            remote(view, view, b_send.at[mask], b_recv.at[mask], {"tp": t2})
        )

    group_masks = [range(g * per_group, (g + 1) * per_group) for g in range(group_count)]
    w_copy = {}

    def send_down(mask, e):
        w_copy[mask, e] = start(
            remote(
                down_hbm.at[e, :, window(flip(t, mask))],
                dcols.at[e, unit_window(t), :],
                w_send.at[mask, e],
                w_recv.at[mask, e],
                {"tp": flip(t, mask)},
            )
        )

    for mask in (2, 1):
        for e in range(local_experts):
            send_down(mask, e)
    loads["tokens"].wait()
    strip = 32

    def normalize(i, carry):
        which, first = i // (part_rows // strip), i % (part_rows // strip)
        at = pl.ds(pl.multiple_of(first * strip, strip), strip)
        to = pl.ds(pl.multiple_of(i * strip, strip), strip)
        full = part[which, at, :].astype(F32)
        mean = jnp.mean(full * full, axis=1, keepdims=True)
        inverse = lax.rsqrt(mean + EPSILON)
        for k, owner in enumerate((t, t2)):
            piece = part[which, at, window(owner)].astype(F32)
            nb[k][to, :] = (piece * inverse * gain_ref[:, window(owner)]).astype(BF16)
        return carry

    lax.fori_loop(0, token_count // strip, normalize, 0)
    line = lax.broadcasted_iota(jnp.int32, (LANES, token_count), 0)
    raw_sum = raw_ref[0:1, :] + raw_ref[1:2, :]
    packed = jnp.zeros((LANES, token_count), F32)
    for j in range(2):
        share = likelihood_ref[...] * (raw_ref[j : j + 1, :] / raw_sum)
        packed = jnp.where(line == j, choice_ref[j : j + 1, :].astype(F32), packed)
        packed = jnp.where(line == 2 + j, share, packed)
    placed = jnp.transpose(packed)
    lane = lax.broadcasted_iota(jnp.int32, (token_count, LANES), 1).astype(F32)
    named = [placed[:, j : j + 1] == lane for j in range(2)]
    counted = sum(jnp.where(mask, 1.0, 0.0) for mask in named).astype(BF16)
    earlier = lax.broadcasted_iota(
        jnp.int32, (token_count, token_count), 0
    ) > lax.broadcasted_iota(jnp.int32, (token_count, token_count), 1)
    before = dot(jnp.where(earlier, 1.0, 0.0).astype(BF16), counted)
    for j in range(2):
        rank = jnp.sum(jnp.where(named[j], before, 0.0), axis=1, keepdims=True)
        placed = jnp.where(lane == 4 + j, placed[:, j : j + 1] * cap + rank, placed)
    route_col[...] = placed
    slot_row[...] = jnp.transpose(placed)[0:8, :]

    dispatch(group_masks[2][0])
    for mask in group_masks[0]:
        if mask:
            dispatch(mask)

    TQ, TC, TW1, TW2, TF, TWI, TWL = range(7)
    stable = jnp.full((1, LANES), FLOOR_LOG, F32)
    total = jnp.zeros((1, LANES), F32)
    for b in range(block_count):
        span, peak = gp_ref[0, b : b + 1, :], gp_ref[1, b : b + 1, :]
        tabs[TQ, b : b + 1, :] = total
        tabs[TC, b : b + 1, :] = stable
        newer = jnp.maximum(span + stable, peak)
        tabs[TW1, b : b + 1, :] = jnp.exp(span + stable - newer)
        tabs[TW2, b : b + 1, :] = jnp.exp(peak - newer)
        stable, total = newer, total + span
    stat[0:1, :] = stable
    stat[1:2, :] = total
    stats[me, 0:1, :] = stable
    stats[me, 1:2, :] = total

    loads["k"].wait()
    loads["v"].wait()
    cst[0] = jnp.zeros(cst.shape[1:], F32)

    def gather_block(b, carry):
        at = pl.ds(pl.multiple_of(b * BLOCK, BLOCK), BLOCK)
        for h in range(head_count):
            keyed = kb[at, h * key_width : (h + 1) * key_width].astype(F32)
            weight = cols_ref[at, head_count + h : head_count + h + 1]
            update = dot(
                (keyed * weight).astype(BF16),
                vb[at, h * value_width : (h + 1) * value_width],
                ((0,), (0,)),
            )
            old = tabs[TW1, pl.ds(b, 1), h : h + 1]
            new = tabs[TW2, pl.ds(b, 1), h : h + 1]
            cst[b + 1, h] = old * cst[b, h] + new * update
        return carry

    lax.fori_loop(0, block_count, gather_block, 0)
    st_buf[slot] = cst[block_count].astype(BF16)
    s_copy = {
        mask: start(
            remote(stat, stats.at[me], s_send.at[mask], s_recv.at[mask], peer(mask))
        )
        for mask in range(1, n)
    }
    t_copy = {
        mask: start(
            remote(
                st_buf.at[slot], st_buf.at[slot], t_send.at[mask], t_recv.at[mask], peer(mask))
        )
        for mask in range(1, half)
    }
    for mask in group_masks[2][1:]:
        dispatch(mask)
    for mask in group_masks[1][: per_group // 2]:
        dispatch(mask)

    keep_own()
    for mask in range(1, n):
        s_copy[mask].wait_recv()
    for mask in range(1, half):
        t_copy[mask].wait_recv()

    low_log, suffix = [None] * half, jnp.zeros((1, LANES), F32)
    for j in reversed(range(half)):
        low_log[j] = stats[j, 0:1, :] + suffix
        suffix = suffix + stats[j, 1:2, :]
    low_stable = functools.reduce(jnp.maximum, low_log)
    low_weight = [jnp.exp(value - low_stable) for value in low_log]

    l_copy = remote(
        low_send, low_buf, l_send.at[0], l_recv.at[0], {"ep": flip(me, half)}
    )

    @pl.when(me < half)
    def _():
        for h in range(head_count):
            summed = jnp.zeros((key_width, value_width), F32)
            for j in range(half):
                summed = summed + low_weight[j][:, h : h + 1] * st_buf[j, h].astype(F32)
            low_send[h] = summed.astype(BF16)
        low_buf[...] = jnp.zeros(low_buf.shape, BF16)
        l_copy.start()

    for mask in group_masks[3]:
        dispatch(mask)
    for mask in group_masks[1][per_group // 2 :]:
        dispatch(mask)

    for i, mask in enumerate(group_masks[2]):
        forward_x(mask)
        for e in range(i, local_experts if i + 1 == per_group else min(i + 1, local_experts)):
            send_down(3, e)

    logs, valid, suffix = [None] * half, [None] * half, jnp.zeros((1, LANES), F32)
    for j in reversed(range(half)):
        valid[j] = j < slot
        logs[j] = jnp.where(valid[j], stats[base + j, 0:1, :] + suffix, FLOOR_LOG)
        suffix = jnp.where(valid[j], suffix + stats[base + j, 1:2, :], suffix)
    low_in = jnp.where(me >= half, low_stable + suffix, FLOOR_LOG)
    peak_in = functools.reduce(jnp.maximum, logs + [low_in])
    weights = [
        jnp.where(valid[j], jnp.exp(logs[j] - peak_in), 0.0) for j in range(half)
    ]
    low_in = jnp.where(me >= half, jnp.exp(low_in - peak_in), 0.0)
    carried_stable = tabs[TQ] + peak_in
    full_stable = jnp.maximum(carried_stable, tabs[TC])
    tabs[TF] = full_stable
    tabs[TWI] = jnp.exp(carried_stable - full_stable)
    tabs[TWL] = jnp.exp(tabs[TC] - full_stable)

    @pl.when(me >= half)
    def _():
        l_copy.wait_recv()

    for h in range(head_count):
        summed = low_in[:, h : h + 1] * low_buf[h].astype(F32)
        for j in range(half):
            summed = summed + weights[j][:, h : h + 1] * st_buf[j, h].astype(F32)
        cst[0, h] = summed

    loads["q"].wait()
    scale = 1.0 / math.sqrt(key_width)
    causal = lax.broadcasted_iota(jnp.int32, (BLOCK, BLOCK), 0) >= lax.broadcasted_iota(
        jnp.int32, (BLOCK, BLOCK), 1
    )

    def read_block(b, carry):
        at = pl.ds(pl.multiple_of(b * BLOCK, BLOCK), BLOCK)
        for h in range(head_count):
            query = qb[at, h * key_width : (h + 1) * key_width]
            key = kb[at, h * key_width : (h + 1) * key_width]
            value = vb[at, h * value_width : (h + 1) * value_width]
            running = cols_ref[at, h : h + 1]
            other = arow_ref[pl.ds(h * block_count + b, 1), :]
            scores = dot(query, key, ((1,), (1,))) * scale
            log_weight = jnp.where(causal, running + other, FLOOR_LOG)
            carried = running + tabs[TF, pl.ds(b, 1), h : h + 1]
            highest = jnp.maximum(carried, jnp.max(log_weight, axis=1, keepdims=True))
            inner = (scores * jnp.exp(log_weight - highest)).astype(BF16)
            memory = (
                tabs[TWI, pl.ds(b, 1), h : h + 1] * cst[0, h]
                + tabs[TWL, pl.ds(b, 1), h : h + 1] * cst[b, h]
            ).astype(BF16)
            state = jnp.exp(carried - highest) * dot(query, memory) + dot(inner, value)
            mean = jnp.mean(state * state, axis=1, keepdims=True)
            state = state * lax.rsqrt(mean + EPSILON)
            at_head = slice(h * value_width, (h + 1) * value_width)
            hid[at, at_head] = (state * hscale_ref[:, at_head]).astype(BF16)
        return carry

    lax.fori_loop(0, block_count, read_block, 0)

    loads["wo"].wait()

    def project(index):
        left = hid[pl.ds(pl.multiple_of(index * part_rows, part_rows), part_rows), :]

        def piece(i, carry):
            at = pl.ds(pl.multiple_of(i * wide, wide), wide)
            part[index, :, at] = dot(left, wo[:, at]).astype(BF16)
            return carry

        lax.fori_loop(0, model // wide, piece, 0)

    m_copy = []
    for i in range(2):
        project(2 * i + 1 - core)
        m_copy.append(
            start(
                remote(
                    part.at[2 * i + 1 - core],
                    crecv.at[i],
                    m_send.at[i],
                    m_recv.at[i],
                    {"tp": t1},
                )
            )
        )
    project(t2)
    forward_x(group_masks[3][0])
    chunk = 32

    def add_other(i, carry):
        at = pl.ds(pl.multiple_of(i * chunk, chunk), chunk)
        part[t2, at, :] = (
            part[t2, at, :].astype(F32) + crecv[1 - side, at, :].astype(F32)
        ).astype(BF16)
        return carry

    f_copy, h_copy = {}, {}

    def stage_core(g, which):
        if which == 0:
            for mask in group_masks[g]:
                if 0 < mask < half:
                    a_copy[mask].wait_recv()
        else:
            for mask in group_masks[g]:
                if mask:
                    b_copy[mask].wait_recv()
        view = rows.at[
            :, slots(group_masks[g][0], per_group), window(t if which == 0 else t2)
        ]
        f_copy[g, which] = start(
            remote(view, view, f_send.at[which, g], f_recv.at[which, g], {"tp": t1})
        )

    def group_slots(g):
        return slots(group_masks[g][0], per_group)

    def send_units(g, kind, owner, target):
        view = fh.at[:, group_slots(g), unit_window(owner)]
        h_copy[g, kind] = start(
            remote(view, view, h_send.at[kind, g], h_recv.at[kind, g], {"tp": target})
        )

    weights_ready = []

    def stage_hidden(g):
        f_copy[g, 0].wait_recv()
        f_copy[g, 1].wait_recv()
        if not weights_ready:
            loads["gate"].wait()
            loads["up"].wait()
            weights_ready.append(True)

        def one(e, carry):
            left = rows[e, group_slots(g), :]
            gate = dot(left, gw[e])
            upward = dot(left, uw[e])
            fh[e, group_slots(g), unit_window(t)] = (
                gate * jax.nn.sigmoid(gate) * upward
            ).astype(BF16)
            return carry

        lax.fori_loop(0, local_experts, one, 0)
        send_units(g, 0, t, t2)
        send_units(g, 1, t, t1)

    def stage_units(g):
        h_copy[g, 0].wait_recv()
        send_units(g, 2, t2, t1)

    down_ready = []
    r_copy = {}

    def stage_down(g):
        h_copy[g, 1].wait_recv()
        h_copy[g, 2].wait_recv()
        if not down_ready:
            loads["down"].wait()
            for copy in w_copy.values():
                copy.wait_recv()
            down_ready.append(True)
        for mask in group_masks[g]:
            if mask:
                a_copy[mask].wait_send()
                sent.add(id(a_copy[mask]))

        def one(i, carry):
            e, c = i // (width // tile), i % (width // tile)
            at = pl.ds(pl.multiple_of(c * tile, tile), tile)
            res[e, group_slots(g), at] = dot(
                fh[e, group_slots(g), :], dcols[e, :, at]
            ).astype(BF16)
            return carry

        lax.fori_loop(0, local_experts * (width // tile), one, 0)
        for mask in group_masks[g]:
            view = res.at[:, slots(mask), :]
            if mask:
                r_copy[mask] = start(
                    remote(
                        view,
                        ret.at[:, slots(mask), :],
                        r_send.at[mask],
                        r_recv.at[mask],
                        peer(mask),
                    )
                )
            else:
                load("ret", view, ret.at[:, slots(0), :])

    x_copy = []
    pieces = 4

    def send_mixed(i):
        at = pl.ds(i * (part_rows // pieces), part_rows // pieces)
        x_copy.append(
            start(
                remote(
                    part.at[t2, at],
                    xrecv.at[at],
                    m_send.at[2 + i],
                    m_recv.at[2 + i],
                    {"tp": t2},
                )
            )
        )

    stage_core(2, 0)
    stage_core(2, 1)
    stage_core(0, 0)
    stage_core(0, 1)
    stage_hidden(2)
    stage_hidden(0)
    for copy in m_copy:
        copy.wait_recv()
    lax.fori_loop(0, part_rows // chunk, add_other, 0)
    send_mixed(0)
    stage_units(2)
    stage_down(2)
    for mask in group_masks[3][1:]:
        forward_x(mask)
    stage_units(0)
    stage_down(0)
    stage_core(3, 0)
    stage_core(1, 0)
    stage_core(1, 1)
    stage_core(3, 1)
    stage_hidden(3)
    send_mixed(1)
    stage_hidden(1)
    send_mixed(2)
    send_mixed(3)
    stage_units(3)
    stage_down(3)
    project(t)
    stage_units(1)
    stage_down(1)
    def add_own(i, carry):
        at = pl.ds(pl.multiple_of(i * chunk, chunk), chunk)
        xrecv[at, :] = (
            part[t, at, :].astype(F32)
            + crecv[side, at, :].astype(F32)
            + xrecv[at, :].astype(F32)
        ).astype(BF16)
        return carry

    across = width // tile

    def combine(g, first, last):
        for mask in group_masks[g]:
            if mask:
                r_copy[mask].wait_recv()
            else:
                loads["ret"].wait()
        length = per_group * cap
        place = lax.broadcasted_iota(jnp.int32, (BLOCK, length), 1)
        ids = []
        for e in range(local_experts):
            found = jnp.zeros((BLOCK, length), jnp.int32)
            for i, mask in enumerate(group_masks[g]):
                begin = (flip(me, mask) * local_experts + e) * cap - i * cap
                found = jnp.where(place >= i * cap, place + begin, found)
            ids.append(found.astype(F32))

        def row_tile(i, carry):
            at = pl.ds(pl.multiple_of(i * BLOCK, BLOCK), BLOCK)
            picks = []
            for e in range(local_experts):
                found = [
                    jnp.where(route_col[at, 4 + j : 5 + j] == ids[e], 1.0, 0.0) for j in range(2)
                ]
                picks.append(jnp.concatenate(found, axis=0).astype(BF16))
            for j in range(across):
                cut = slice(j * tile, (j + 1) * tile)
                both = sum(
                    dot(picks[e], ret[e, group_slots(g), cut]) for e in range(local_experts)
                )
                total = route_col[at, 2:3] * both[:BLOCK] + route_col[at, 3:4] * both[BLOCK:]
                where = i * across + j
                held = (where // head_count, where % head_count)
                if not first:
                    total = total + cst[held[0], held[1]]
                if last:
                    routed_ref[at, cut] = total.astype(BF16)
                else:
                    cst[held[0], held[1]] = total
            return carry

        lax.fori_loop(0, token_count // BLOCK, row_tile, 0)

    combine(0, True, False)
    combine(2, False, False)
    combine(1, False, False)
    for copy in x_copy:
        copy.wait_recv()
    lax.fori_loop(0, part_rows // chunk, add_own, 0)
    combine(3, False, True)
    for copy in sends:
        if id(copy) not in sent:
            copy.wait_send()

    @pl.when(me < half)
    def _():
        l_copy.wait_send()


def gates(log_input_gate, forget_preactivation, forget_offset, key_width):
    row_count, head_count = log_input_gate.shape
    block_count = row_count // BLOCK
    forget_log = jax.nn.log_sigmoid(forget_preactivation) + forget_offset
    forget_log = forget_log.reshape(block_count, BLOCK, head_count)
    in_gate = log_input_gate.reshape(block_count, BLOCK, head_count)
    lower = jnp.tril(jnp.ones((BLOCK, BLOCK), F32))
    running = jnp.einsum(
        "ts,bsh->bth",
        lower,
        forget_log,
        preferred_element_type=F32,
        precision=lax.Precision.HIGHEST,
    )
    totals = running[:, -1]
    to_end = totals[:, None] - running + in_gate
    peak = jnp.max(to_end, axis=1)
    key_weight = jnp.exp(to_end - peak[:, None]) * (1.0 / math.sqrt(key_width))
    cols = jnp.concatenate([running, key_weight], axis=2).reshape(row_count, -1)
    arow = (in_gate - running).transpose(2, 0, 1).reshape(head_count * block_count, BLOCK)
    gp = jnp.pad(jnp.stack([totals, peak]), ((0, 0), (0, 0), (0, LANES - head_count)))
    return cols, arow, gp


def per_device(
    queries,
    keys,
    values,
    log_input_gate,
    forget_preactivation,
    forget_offset,
    head_norm_scale,
    memory_output_weight,
    second_micro_tokens,
    expert_norm_scale,
    expert_choice_index,
    group_likelihood,
    expert_raw_weight,
    gate_weight,
    up_weight,
    down_weight,
):
    token_count, model_width = second_micro_tokens.shape
    pick_count = expert_choice_index.shape[1]
    local_experts, _, units = gate_weight.shape
    n, tp = lax.axis_size("ep"), lax.axis_size("tp")
    half = n // 2
    expert_count = local_experts * n
    cap = tp * max(1, 3 * pick_count * token_count // (2 * expert_count * tp))
    width = model_width // tp
    row_count, head_count = log_input_gate.shape
    key_width = queries.shape[1] // head_count
    value_width = values.shape[1] // head_count
    block_count = row_count // BLOCK
    out_depth = head_count * value_width

    cols, arow, gp = gates(log_input_gate, forget_preactivation, forget_offset, key_width)

    slot_rows = n * cap
    part_rows = row_count // tp
    vmem = pl.BlockSpec(memory_space=pltpu.VMEM)
    hbm = pl.BlockSpec(memory_space=pl.ANY)
    dma = pltpu.SemaphoreType.DMA
    mixed, routed = pl.pallas_call(
        functools.partial(kernel, n, tp, cap),
        out_shape=(
            jax.ShapeDtypeStruct((part_rows, model_width), BF16),
            jax.ShapeDtypeStruct((token_count, width), BF16),
        ),
        in_specs=[hbm] + [vmem] * 4 + [hbm] * 3 + [vmem] * 4 + [hbm] * 4,
        out_specs=(vmem, vmem),
        scratch_shapes=[
            pltpu.VMEM((local_experts, slot_rows, model_width), BF16),
            pltpu.VMEM(gate_weight.shape, BF16),
            pltpu.VMEM(up_weight.shape, BF16),
            pltpu.VMEM((local_experts, tp * units, width), BF16),
            pltpu.VMEM((local_experts, slot_rows, tp * units), BF16),
            pltpu.VMEM((local_experts, slot_rows, width), BF16),
            pltpu.VMEM((tp, part_rows, model_width), BF16),
            pltpu.VMEM((2, part_rows, model_width), BF16),
            pltpu.VMEM(queries.shape, BF16),
            pltpu.VMEM(keys.shape, BF16),
            pltpu.VMEM(values.shape, BF16),
            pltpu.VMEM((row_count, out_depth), BF16),
            pltpu.VMEM((out_depth, model_width), BF16),
            pltpu.VMEM((block_count + 1, head_count, key_width, value_width), F32),
            pltpu.VMEM((7, block_count, LANES), F32),
            pltpu.VMEM((8, LANES), F32),
            pltpu.VMEM((n, 8, LANES), F32),
            pltpu.VMEM((half, head_count, key_width, value_width), BF16),
            pltpu.VMEM((head_count, key_width, value_width), BF16),
            pltpu.VMEM((head_count, key_width, value_width), BF16),
            pltpu.VMEM((local_experts, slot_rows, width), BF16),
            pltpu.VMEM((token_count, width), BF16),
            pltpu.VMEM((half - 1, local_experts, cap, width), BF16),
            pltpu.VMEM((token_count, LANES), F32),
            pltpu.VMEM((8, token_count), F32),
            dma((12,)),
            dma((n,)),
            dma((n,)),
            dma((n,)),
            dma((n,)),
            dma((2, 4)),
            dma((2, 4)),
            dma((3, 4)),
            dma((3, 4)),
            dma((tp, local_experts)),
            dma((tp, local_experts)),
            dma((n,)),
            dma((n,)),
            dma((half,)),
            dma((half,)),
            dma((1,)),
            dma((1,)),
            dma((6,)),
            dma((6,)),
            dma((n,)),
            dma((n,)),
        ],
        compiler_params=pltpu.CompilerParams(
            collective_id=0, has_side_effects=True, vmem_limit_bytes=67043328
        ),
        name="exchange",
    )(
        second_micro_tokens.reshape(-1, part_rows, model_width),
        expert_norm_scale.reshape(1, -1),
        expert_choice_index.T,
        group_likelihood.reshape(1, -1),
        expert_raw_weight.T,
        queries,
        keys,
        values,
        cols,
        arow,
        gp,
        head_norm_scale.reshape(1, -1),
        memory_output_weight,
        gate_weight,
        up_weight,
        down_weight,
    )
    return mixed, routed


def solution(mesh):
    in_specs = (
        P("ep", "tp"),
        P("ep", "tp"),
        P("ep", "tp"),
        P("ep", "tp"),
        P("ep", "tp"),
        P("ep", "tp"),
        P("tp"),
        P("tp", None),
        P("ep", None),
        P(),
        P("ep", None),
        P("ep"),
        P("ep", None),
        P("ep", None, "tp"),
        P("ep", None, "tp"),
        P("ep", "tp", None),
    )
    out_specs = (P(("ep", "tp"), None), P("ep", "tp"))
    return jax.shard_map(
        per_device, mesh=mesh, in_specs=in_specs, out_specs=out_specs, check_vma=False
    )
```

```python
import functools
import math

import jax
import jax.numpy as jnp
from jax import lax
from jax.experimental import pallas as pl
from jax.experimental.pallas import tpu as pltpu
from jax.sharding import PartitionSpec as P

BLOCK = 128
EPSILON = 1e-06
FLOOR_LOG = -1e30
LANES = 128
MESH = pl.DeviceIdType.MESH
F32 = jnp.float32
BF16 = jnp.bfloat16


def flip(index, mask):
    bit = 1
    while bit <= mask:
        if mask & bit:
            index = index + bit * (1 - 2 * ((index // bit) % 2))
        bit *= 2
    return index


def dot(left, right, dims=((1,), (0,))):
    return lax.dot_general(left, right, (dims, ((), ())), preferred_element_type=F32)


def kernel(
    n,
    tp,
    cap,
    tok_hbm,
    gain_ref,
    choice_ref,
    likelihood_ref,
    raw_ref,
    q_hbm,
    k_hbm,
    v_hbm,
    in_gate_ref,
    forget_ref,
    offset_ref,
    hscale_ref,
    wo_hbm,
    gate_hbm,
    up_hbm,
    down_hbm,
    xrecv,
    routed_ref,
    rows,
    gw,
    uw,
    dcols,
    fh,
    res,
    part,
    crecv,
    qb,
    kb,
    vb,
    hid,
    wo,
    cst,
    tabs,
    stat,
    stats,
    st_buf,
    low_send,
    low_buf,
    ret,
    other_nb,
    bbuf,
    route_col,
    slot_row,
    arow_ref,
    cols_ref,
    load_sem,
    a_send,
    a_recv,
    b_send,
    b_recv,
    f_send,
    f_recv,
    h_send,
    h_recv,
    w_send,
    w_recv,
    s_send,
    s_recv,
    t_send,
    t_recv,
    l_send,
    l_recv,
    m_send,
    m_recv,
    r_send,
    r_recv,
):
    me, t = lax.axis_index("ep"), lax.axis_index("tp")
    half = n // 2
    group_count = 4
    per_group = n // group_count
    local_experts, _, width = res.shape
    token_count = routed_ref.shape[0]
    nb = (routed_ref, other_nb)
    rows_sent = local_experts * cap
    units = gw.shape[2]
    block_count, head_count = cst.shape[0] - 1, cst.shape[1]
    key_width, value_width = cst.shape[2:]
    row_count = qb.shape[0]
    part_rows = part.shape[1]
    model = rows.shape[2]
    t1, t2 = flip(t, 1), flip(t, 2)
    core, side = t % 2, t // 2
    base = (me // half) * half
    slot = me - base

    def peer(mask):
        return {"ep": flip(me, mask)}

    def window(index):
        return pl.ds(pl.multiple_of(index * width, LANES), width)

    def unit_window(index):
        return pl.ds(pl.multiple_of(index * units, LANES), units)

    def remote(src, dst, send, recv, device):
        return pltpu.make_async_remote_copy(
            src_ref=src,
            dst_ref=dst,
            send_sem=send,
            recv_sem=recv,
            device_id=device,
            device_id_type=MESH,
        )

    barrier = pltpu.get_barrier_semaphore()
    for mask in range(1, n):
        pl.semaphore_signal(barrier, inc=1, device_id=peer(mask), device_id_type=MESH)
    for mask in range(1, tp):
        pl.semaphore_signal(
            barrier, inc=1, device_id={"tp": flip(t, mask)}, device_id_type=MESH
        )

    loads = {}

    def load(name, src, dst):
        loads[name] = pltpu.make_async_copy(src, dst, load_sem.at[len(loads)])
        loads[name].start()

    token_tiles = token_count // part_rows
    load("tokens", tok_hbm, part.at[pl.ds(0, token_tiles)])
    load("k", k_hbm, kb)
    load("v", v_hbm, vb)
    load("q", q_hbm, qb)
    load("wo", wo_hbm, wo)
    load("gate", gate_hbm, gw)
    load("up", up_hbm, uw)
    load("down", down_hbm.at[:, :, window(t)], dcols.at[:, unit_window(t), :])
    pl.semaphore_wait(barrier, n - 1 + tp - 1)

    sends, sent = [], set()
    tile, wide = 256, 512

    def start(copy):
        copy.start()
        sends.append(copy)
        return copy

    def slots(mask, count=1):
        return pl.ds(mask * cap, count * cap)

    a_copy, b_copy = {}, {}

    def select(mask, which, store):
        first = flip(me, mask) * rows_sent
        ids = lax.broadcasted_iota(jnp.int32, (rows_sent, token_count), 0) + first
        ids = ids.astype(F32)
        chosen = (slot_row[4:5, :] == ids) | (slot_row[5:6, :] == ids)
        chosen = jnp.where(chosen, 1.0, 0.0).astype(BF16)

        def piece(i, carry):
            at = pl.multiple_of(i * wide, wide)
            picked = dot(chosen, nb[which][:, pl.ds(at, wide)])
            for e in range(local_experts):
                store(e, at, picked[e * cap : (e + 1) * cap].astype(BF16))
            return carry

        lax.fori_loop(0, width // wide, piece, 0)

    def dispatch(mask):
        def store_a(e, at, value):
            res[e, slots(mask), pl.ds(at, wide)] = value

        def store_b(e, at, value):
            bbuf[mask - 1, e, :, pl.ds(at, wide)] = value

        select(mask, 0, store_a)
        a_copy[mask] = start(
            remote(
                res.at[:, slots(mask), :],
                rows.at[:, slots(mask), window(t)],
                a_send.at[mask],
                a_recv.at[mask],
                peer(mask),
            )
        )
        if mask < half:
            select(mask, 1, store_b)
            b_copy[mask] = start(
                remote(
                    bbuf.at[mask - 1],
                    rows.at[:, slots(mask), window(t2)],
                    b_send.at[mask],
                    b_recv.at[mask],
                    peer(mask),
                )
            )

    def keep_own():
        for which, owner in enumerate((t, t2)):

            def store(e, at, value):
                begin = pl.multiple_of(owner * width + at, wide)
                rows[e, slots(0), pl.ds(begin, wide)] = value

            select(0, which, store)

    def forward_x(mask):
        a_copy[mask].wait_recv()
        view = rows.at[:, slots(mask), window(t)]
        b_copy[mask] = start(
            remote(view, view, b_send.at[mask], b_recv.at[mask], {"tp": t2})
        )

    group_masks = [range(g * per_group, (g + 1) * per_group) for g in range(group_count)]
    w_copy = {}

    def send_down(mask, e):
        w_copy[mask, e] = start(
            remote(
                down_hbm.at[e, :, window(flip(t, mask))],
                dcols.at[e, unit_window(t), :],
                w_send.at[mask, e],
                w_recv.at[mask, e],
                {"tp": flip(t, mask)},
            )
        )

    for mask in (2, 1):
        for e in range(local_experts):
            send_down(mask, e)
    loads["tokens"].wait()
    strip = 32

    def normalize(i, carry):
        which, first = i // (part_rows // strip), i % (part_rows // strip)
        at = pl.ds(pl.multiple_of(first * strip, strip), strip)
        to = pl.ds(pl.multiple_of(i * strip, strip), strip)
        full = part[which, at, :].astype(F32)
        mean = jnp.mean(full * full, axis=1, keepdims=True)
        inverse = lax.rsqrt(mean + EPSILON)
        for k, owner in enumerate((t, t2)):
            piece = part[which, at, window(owner)].astype(F32)
            nb[k][to, :] = (piece * inverse * gain_ref[:, window(owner)]).astype(BF16)
        return carry

    lax.fori_loop(0, token_count // strip, normalize, 0)
    line = lax.broadcasted_iota(jnp.int32, (LANES, token_count), 0)
    raw_sum = raw_ref[0:1, :] + raw_ref[1:2, :]
    packed = jnp.zeros((LANES, token_count), F32)
    for j in range(2):
        share = likelihood_ref[...] * (raw_ref[j : j + 1, :] / raw_sum)
        packed = jnp.where(line == j, choice_ref[j : j + 1, :].astype(F32), packed)
        packed = jnp.where(line == 2 + j, share, packed)
    placed = jnp.transpose(packed)
    lane = lax.broadcasted_iota(jnp.int32, (token_count, LANES), 1).astype(F32)
    named = [placed[:, j : j + 1] == lane for j in range(2)]
    counted = sum(jnp.where(mask, 1.0, 0.0) for mask in named).astype(BF16)
    earlier = lax.broadcasted_iota(
        jnp.int32, (token_count, token_count), 0
    ) > lax.broadcasted_iota(jnp.int32, (token_count, token_count), 1)
    before = dot(jnp.where(earlier, 1.0, 0.0).astype(BF16), counted)
    for j in range(2):
        rank = jnp.sum(jnp.where(named[j], before, 0.0), axis=1, keepdims=True)
        placed = jnp.where(lane == 4 + j, placed[:, j : j + 1] * cap + rank, placed)
    route_col[...] = placed
    slot_row[...] = jnp.transpose(placed)[0:8, :]

    dispatch(group_masks[2][0])
    for mask in group_masks[0]:
        if mask:
            dispatch(mask)

    TQ, TC, TW1, TW2, TF, TWI, TWL = range(7)
    pair_count = block_count * head_count
    scale = 1.0 / math.sqrt(key_width)
    high = lax.Precision.HIGHEST

    def exact(left, right):
        return lax.dot_general(
            left, right, (((1,), (0,)), ((), ())), precision=high, preferred_element_type=F32
        )

    row_at = lax.broadcasted_iota(jnp.int32, (BLOCK, BLOCK), 0)
    lane_at = lax.broadcasted_iota(jnp.int32, (BLOCK, BLOCK), 1)
    forget = forget_ref[...]
    forget_log = jnp.minimum(forget, 0.0) - jnp.log1p(jnp.exp(-jnp.abs(forget)))
    forget_log = forget_log + offset_ref[...]
    running_rows = exact(forget_log, jnp.where(row_at <= lane_at, 1.0, 0.0))
    spans = running_rows[:, BLOCK - 1 : BLOCK]
    to_end = spans - running_rows + in_gate_ref[...]
    peaks = jnp.max(to_end, axis=1, keepdims=True)
    key_rows = jnp.exp(to_end - peaks) * scale
    arow_ref[...] = in_gate_ref[...] - running_rows
    tall = jnp.concatenate(
        [running_rows, key_rows, jnp.zeros((BLOCK - 2 * pair_count, BLOCK), F32)], axis=0
    )
    cols_ref[...] = jnp.transpose(tall)
    pair_row = lax.broadcasted_iota(jnp.int32, (pair_count, LANES), 0)
    pair_lane = lax.broadcasted_iota(jnp.int32, (pair_count, LANES), 1)
    of_head = pair_lane == pair_row % head_count
    block_row = lax.broadcasted_iota(jnp.int32, (block_count, pair_count), 0)
    block_lane = lax.broadcasted_iota(jnp.int32, (block_count, pair_count), 1)
    of_block = jnp.where(block_lane // head_count == block_row, 1.0, 0.0)
    span_table = exact(of_block, jnp.where(of_head, spans, 0.0))
    peak_table = exact(of_block, jnp.where(of_head, peaks, 0.0))

    def column(index):
        return jnp.sum(
            jnp.where(lane_at == index, cols_ref[...], 0.0), axis=1, keepdims=True
        )

    stable = jnp.full((1, LANES), FLOOR_LOG, F32)
    total = jnp.zeros((1, LANES), F32)
    for b in range(block_count):
        span, peak = span_table[b : b + 1, :], peak_table[b : b + 1, :]
        tabs[TQ, b : b + 1, :] = total
        tabs[TC, b : b + 1, :] = stable
        newer = jnp.maximum(span + stable, peak)
        tabs[TW1, b : b + 1, :] = jnp.exp(span + stable - newer)
        tabs[TW2, b : b + 1, :] = jnp.exp(peak - newer)
        stable, total = newer, total + span
    stat[0:1, :] = stable
    stat[1:2, :] = total
    stats[me, 0:1, :] = stable
    stats[me, 1:2, :] = total

    loads["k"].wait()
    loads["v"].wait()
    cst[0] = jnp.zeros(cst.shape[1:], F32)

    def gather_block(b, carry):
        at = pl.ds(pl.multiple_of(b * BLOCK, BLOCK), BLOCK)
        for h in range(head_count):
            keyed = kb[at, h * key_width : (h + 1) * key_width].astype(F32)
            weight = column(pair_count + b * head_count + h)
            update = dot(
                (keyed * weight).astype(BF16),
                vb[at, h * value_width : (h + 1) * value_width],
                ((0,), (0,)),
            )
            old = tabs[TW1, pl.ds(b, 1), h : h + 1]
            new = tabs[TW2, pl.ds(b, 1), h : h + 1]
            cst[b + 1, h] = old * cst[b, h] + new * update
        return carry

    lax.fori_loop(0, block_count, gather_block, 0)
    st_buf[slot] = cst[block_count].astype(BF16)
    s_copy = {
        mask: start(
            remote(stat, stats.at[me], s_send.at[mask], s_recv.at[mask], peer(mask))
        )
        for mask in range(1, n)
    }
    t_copy = {
        mask: start(
            remote(
                st_buf.at[slot], st_buf.at[slot], t_send.at[mask], t_recv.at[mask], peer(mask))
        )
        for mask in range(1, half)
    }
    for mask in group_masks[2][1:]:
        dispatch(mask)
    for mask in group_masks[1][: per_group // 2]:
        dispatch(mask)

    keep_own()
    for mask in range(1, n):
        s_copy[mask].wait_recv()
    for mask in range(1, half):
        t_copy[mask].wait_recv()

    low_log, suffix = [None] * half, jnp.zeros((1, LANES), F32)
    for j in reversed(range(half)):
        low_log[j] = stats[j, 0:1, :] + suffix
        suffix = suffix + stats[j, 1:2, :]
    low_stable = functools.reduce(jnp.maximum, low_log)
    low_weight = [jnp.exp(value - low_stable) for value in low_log]

    l_copy = remote(
        low_send, low_buf, l_send.at[0], l_recv.at[0], {"ep": flip(me, half)}
    )

    @pl.when(me < half)
    def _():
        for h in range(head_count):
            summed = jnp.zeros((key_width, value_width), F32)
            for j in range(half):
                summed = summed + low_weight[j][:, h : h + 1] * st_buf[j, h].astype(F32)
            low_send[h] = summed.astype(BF16)
        low_buf[...] = jnp.zeros(low_buf.shape, BF16)
        l_copy.start()

    for mask in group_masks[3]:
        dispatch(mask)
    for mask in group_masks[1][per_group // 2 :]:
        dispatch(mask)

    for i, mask in enumerate(group_masks[2]):
        forward_x(mask)
        for e in range(i, local_experts if i + 1 == per_group else min(i + 1, local_experts)):
            send_down(3, e)

    logs, valid, suffix = [None] * half, [None] * half, jnp.zeros((1, LANES), F32)
    for j in reversed(range(half)):
        valid[j] = j < slot
        logs[j] = jnp.where(valid[j], stats[base + j, 0:1, :] + suffix, FLOOR_LOG)
        suffix = jnp.where(valid[j], suffix + stats[base + j, 1:2, :], suffix)
    low_in = jnp.where(me >= half, low_stable + suffix, FLOOR_LOG)
    peak_in = functools.reduce(jnp.maximum, logs + [low_in])
    weights = [
        jnp.where(valid[j], jnp.exp(logs[j] - peak_in), 0.0) for j in range(half)
    ]
    low_in = jnp.where(me >= half, jnp.exp(low_in - peak_in), 0.0)
    carried_stable = tabs[TQ] + peak_in
    full_stable = jnp.maximum(carried_stable, tabs[TC])
    tabs[TF] = full_stable
    tabs[TWI] = jnp.exp(carried_stable - full_stable)
    tabs[TWL] = jnp.exp(tabs[TC] - full_stable)

    @pl.when(me >= half)
    def _():
        l_copy.wait_recv()

    for h in range(head_count):
        summed = low_in[:, h : h + 1] * low_buf[h].astype(F32)
        for j in range(half):
            summed = summed + weights[j][:, h : h + 1] * st_buf[j, h].astype(F32)
        cst[0, h] = summed

    loads["q"].wait()
    causal = row_at >= lane_at

    def read_block(b, carry):
        at = pl.ds(pl.multiple_of(b * BLOCK, BLOCK), BLOCK)
        for h in range(head_count):
            query = qb[at, h * key_width : (h + 1) * key_width]
            key = kb[at, h * key_width : (h + 1) * key_width]
            value = vb[at, h * value_width : (h + 1) * value_width]
            running = column(b * head_count + h)
            other = arow_ref[pl.ds(b * head_count + h, 1), :]
            scores = dot(query, key, ((1,), (1,))) * scale
            log_weight = jnp.where(causal, running + other, FLOOR_LOG)
            carried = running + tabs[TF, pl.ds(b, 1), h : h + 1]
            highest = jnp.maximum(carried, jnp.max(log_weight, axis=1, keepdims=True))
            inner = (scores * jnp.exp(log_weight - highest)).astype(BF16)
            memory = (
                tabs[TWI, pl.ds(b, 1), h : h + 1] * cst[0, h]
                + tabs[TWL, pl.ds(b, 1), h : h + 1] * cst[b, h]
            ).astype(BF16)
            state = jnp.exp(carried - highest) * dot(query, memory) + dot(inner, value)
            mean = jnp.mean(state * state, axis=1, keepdims=True)
            state = state * lax.rsqrt(mean + EPSILON)
            at_head = slice(h * value_width, (h + 1) * value_width)
            hid[at, at_head] = (state * hscale_ref[:, at_head]).astype(BF16)
        return carry

    lax.fori_loop(0, block_count, read_block, 0)

    loads["wo"].wait()

    def project(index):
        left = hid[pl.ds(pl.multiple_of(index * part_rows, part_rows), part_rows), :]

        def piece(i, carry):
            at = pl.ds(pl.multiple_of(i * wide, wide), wide)
            part[index, :, at] = dot(left, wo[:, at]).astype(BF16)
            return carry

        lax.fori_loop(0, model // wide, piece, 0)

    m_copy = []
    for i in range(2):
        project(2 * i + 1 - core)
        m_copy.append(
            start(
                remote(
                    part.at[2 * i + 1 - core],
                    crecv.at[i],
                    m_send.at[i],
                    m_recv.at[i],
                    {"tp": t1},
                )
            )
        )
    project(t2)
    forward_x(group_masks[3][0])
    chunk = 32

    def add_other(i, carry):
        at = pl.ds(pl.multiple_of(i * chunk, chunk), chunk)
        part[t2, at, :] = (
            part[t2, at, :].astype(F32) + crecv[1 - side, at, :].astype(F32)
        ).astype(BF16)
        return carry

    f_copy, h_copy = {}, {}

    def stage_core(g, which):
        if which == 0:
            for mask in group_masks[g]:
                if 0 < mask < half:
                    a_copy[mask].wait_recv()
        else:
            for mask in group_masks[g]:
                if mask:
                    b_copy[mask].wait_recv()
        view = rows.at[
            :, slots(group_masks[g][0], per_group), window(t if which == 0 else t2)
        ]
        f_copy[g, which] = start(
            remote(view, view, f_send.at[which, g], f_recv.at[which, g], {"tp": t1})
        )

    def group_slots(g):
        return slots(group_masks[g][0], per_group)

    def send_units(g, kind, owner, target):
        view = fh.at[:, group_slots(g), unit_window(owner)]
        h_copy[g, kind] = start(
            remote(view, view, h_send.at[kind, g], h_recv.at[kind, g], {"tp": target})
        )

    weights_ready = []

    def stage_hidden(g):
        f_copy[g, 0].wait_recv()
        f_copy[g, 1].wait_recv()
        if not weights_ready:
            loads["gate"].wait()
            loads["up"].wait()
            weights_ready.append(True)

        def one(e, carry):
            left = rows[e, group_slots(g), :]
            gate = dot(left, gw[e])
            upward = dot(left, uw[e])
            fh[e, group_slots(g), unit_window(t)] = (
                gate * jax.nn.sigmoid(gate) * upward
            ).astype(BF16)
            return carry

        lax.fori_loop(0, local_experts, one, 0)
        send_units(g, 0, t, t2)
        send_units(g, 1, t, t1)

    def stage_units(g):
        h_copy[g, 0].wait_recv()
        send_units(g, 2, t2, t1)

    down_ready = []
    r_copy = {}

    def stage_down(g):
        h_copy[g, 1].wait_recv()
        h_copy[g, 2].wait_recv()
        if not down_ready:
            loads["down"].wait()
            for copy in w_copy.values():
                copy.wait_recv()
            down_ready.append(True)
        for mask in group_masks[g]:
            if mask:
                a_copy[mask].wait_send()
                sent.add(id(a_copy[mask]))

        def one(i, carry):
            e, c = i // (width // tile), i % (width // tile)
            at = pl.ds(pl.multiple_of(c * tile, tile), tile)
            res[e, group_slots(g), at] = dot(
                fh[e, group_slots(g), :], dcols[e, :, at]
            ).astype(BF16)
            return carry

        lax.fori_loop(0, local_experts * (width // tile), one, 0)
        for mask in group_masks[g]:
            view = res.at[:, slots(mask), :]
            if mask:
                r_copy[mask] = start(
                    remote(
                        view,
                        ret.at[:, slots(mask), :],
                        r_send.at[mask],
                        r_recv.at[mask],
                        peer(mask),
                    )
                )
            else:
                load("ret", view, ret.at[:, slots(0), :])

    x_copy = []
    pieces = 4

    def send_mixed(i):
        at = pl.ds(i * (part_rows // pieces), part_rows // pieces)
        x_copy.append(
            start(
                remote(
                    part.at[t2, at],
                    xrecv.at[at],
                    m_send.at[2 + i],
                    m_recv.at[2 + i],
                    {"tp": t2},
                )
            )
        )

    stage_core(2, 0)
    stage_core(2, 1)
    stage_core(0, 0)
    stage_core(0, 1)
    stage_hidden(2)
    stage_hidden(0)
    for copy in m_copy:
        copy.wait_recv()
    lax.fori_loop(0, part_rows // chunk, add_other, 0)
    stage_units(2)
    stage_down(2)
    for mask in group_masks[3][1:]:
        forward_x(mask)
    send_mixed(0)
    stage_units(0)
    stage_down(0)
    stage_core(3, 0)
    stage_core(1, 0)
    stage_core(1, 1)
    stage_core(3, 1)
    stage_hidden(3)
    send_mixed(1)
    stage_hidden(1)
    send_mixed(2)
    send_mixed(3)
    stage_units(3)
    stage_down(3)
    project(t)
    stage_units(1)
    stage_down(1)
    def add_own(i, carry):
        at = pl.ds(pl.multiple_of(i * chunk, chunk), chunk)
        xrecv[at, :] = (
            part[t, at, :].astype(F32)
            + crecv[side, at, :].astype(F32)
            + xrecv[at, :].astype(F32)
        ).astype(BF16)
        return carry

    across = width // tile

    def combine(g, first, last):
        for mask in group_masks[g]:
            if mask:
                r_copy[mask].wait_recv()
            else:
                loads["ret"].wait()
        length = per_group * cap
        place = lax.broadcasted_iota(jnp.int32, (BLOCK, length), 1)
        ids = []
        for e in range(local_experts):
            found = jnp.zeros((BLOCK, length), jnp.int32)
            for i, mask in enumerate(group_masks[g]):
                begin = (flip(me, mask) * local_experts + e) * cap - i * cap
                found = jnp.where(place >= i * cap, place + begin, found)
            ids.append(found.astype(F32))

        def row_tile(i, carry):
            at = pl.ds(pl.multiple_of(i * BLOCK, BLOCK), BLOCK)
            picks = []
            for e in range(local_experts):
                found = [
                    jnp.where(route_col[at, 4 + j : 5 + j] == ids[e], 1.0, 0.0) for j in range(2)
                ]
                picks.append(jnp.concatenate(found, axis=0).astype(BF16))
            for j in range(across):
                cut = slice(j * tile, (j + 1) * tile)
                both = sum(
                    dot(picks[e], ret[e, group_slots(g), cut]) for e in range(local_experts)
                )
                total = route_col[at, 2:3] * both[:BLOCK] + route_col[at, 3:4] * both[BLOCK:]
                where = i * across + j
                held = (where // head_count, where % head_count)
                if not first:
                    total = total + cst[held[0], held[1]]
                if last:
                    routed_ref[at, cut] = total.astype(BF16)
                else:
                    cst[held[0], held[1]] = total
            return carry

        lax.fori_loop(0, token_count // BLOCK, row_tile, 0)

    combine(0, True, False)
    combine(2, False, False)
    combine(1, False, False)
    for copy in x_copy:
        copy.wait_recv()
    lax.fori_loop(0, part_rows // chunk, add_own, 0)
    combine(3, False, True)
    for copy in sends:
        if id(copy) not in sent:
            copy.wait_send()

    @pl.when(me < half)
    def _():
        l_copy.wait_send()


def by_block(gate):
    row_count, head_count = gate.shape
    gate = gate.reshape(row_count // BLOCK, BLOCK, head_count).transpose(0, 2, 1)
    return gate.reshape(-1, BLOCK)


def per_device(
    queries,
    keys,
    values,
    log_input_gate,
    forget_preactivation,
    forget_offset,
    head_norm_scale,
    memory_output_weight,
    second_micro_tokens,
    expert_norm_scale,
    expert_choice_index,
    group_likelihood,
    expert_raw_weight,
    gate_weight,
    up_weight,
    down_weight,
):
    token_count, model_width = second_micro_tokens.shape
    pick_count = expert_choice_index.shape[1]
    local_experts, _, units = gate_weight.shape
    n, tp = lax.axis_size("ep"), lax.axis_size("tp")
    half = n // 2
    expert_count = local_experts * n
    cap = tp * max(1, 3 * pick_count * token_count // (2 * expert_count * tp))
    width = model_width // tp
    row_count, head_count = log_input_gate.shape
    key_width = queries.shape[1] // head_count
    value_width = values.shape[1] // head_count
    block_count = row_count // BLOCK
    out_depth = head_count * value_width

    slot_rows = n * cap
    part_rows = row_count // tp
    vmem = pl.BlockSpec(memory_space=pltpu.VMEM)
    hbm = pl.BlockSpec(memory_space=pl.ANY)
    dma = pltpu.SemaphoreType.DMA
    mixed, routed = pl.pallas_call(
        functools.partial(kernel, n, tp, cap),
        out_shape=(
            jax.ShapeDtypeStruct((part_rows, model_width), BF16),
            jax.ShapeDtypeStruct((token_count, width), BF16),
        ),
        in_specs=[hbm] + [vmem] * 4 + [hbm] * 3 + [vmem] * 4 + [hbm] * 4,
        out_specs=(vmem, vmem),
        scratch_shapes=[
            pltpu.VMEM((local_experts, slot_rows, model_width), BF16),
            pltpu.VMEM(gate_weight.shape, BF16),
            pltpu.VMEM(up_weight.shape, BF16),
            pltpu.VMEM((local_experts, tp * units, width), BF16),
            pltpu.VMEM((local_experts, slot_rows, tp * units), BF16),
            pltpu.VMEM((local_experts, slot_rows, width), BF16),
            pltpu.VMEM((tp, part_rows, model_width), BF16),
            pltpu.VMEM((2, part_rows, model_width), BF16),
            pltpu.VMEM(queries.shape, BF16),
            pltpu.VMEM(keys.shape, BF16),
            pltpu.VMEM(values.shape, BF16),
            pltpu.VMEM((row_count, out_depth), BF16),
            pltpu.VMEM((out_depth, model_width), BF16),
            pltpu.VMEM((block_count + 1, head_count, key_width, value_width), F32),
            pltpu.VMEM((7, block_count, LANES), F32),
            pltpu.VMEM((8, LANES), F32),
            pltpu.VMEM((n, 8, LANES), F32),
            pltpu.VMEM((half, head_count, key_width, value_width), BF16),
            pltpu.VMEM((head_count, key_width, value_width), BF16),
            pltpu.VMEM((head_count, key_width, value_width), BF16),
            pltpu.VMEM((local_experts, slot_rows, width), BF16),
            pltpu.VMEM((token_count, width), BF16),
            pltpu.VMEM((half - 1, local_experts, cap, width), BF16),
            pltpu.VMEM((token_count, LANES), F32),
            pltpu.VMEM((8, token_count), F32),
            pltpu.VMEM((block_count * head_count, BLOCK), F32),
            pltpu.VMEM((BLOCK, BLOCK), F32),
            dma((12,)),
            dma((n,)),
            dma((n,)),
            dma((n,)),
            dma((n,)),
            dma((2, 4)),
            dma((2, 4)),
            dma((3, 4)),
            dma((3, 4)),
            dma((tp, local_experts)),
            dma((tp, local_experts)),
            dma((n,)),
            dma((n,)),
            dma((half,)),
            dma((half,)),
            dma((1,)),
            dma((1,)),
            dma((6,)),
            dma((6,)),
            dma((n,)),
            dma((n,)),
        ],
        compiler_params=pltpu.CompilerParams(
            collective_id=0, has_side_effects=True, vmem_limit_bytes=67043328
        ),
        name="exchange",
    )(
        second_micro_tokens.reshape(-1, part_rows, model_width),
        expert_norm_scale.reshape(1, -1),
        expert_choice_index.T,
        group_likelihood.reshape(1, -1),
        expert_raw_weight.T,
        queries,
        keys,
        values,
        by_block(log_input_gate),
        by_block(forget_preactivation),
        by_block(forget_offset),
        head_norm_scale.reshape(1, -1),
        memory_output_weight,
        gate_weight,
        up_weight,
        down_weight,
    )
    return mixed, routed


def solution(mesh):
    in_specs = (
        P("ep", "tp"),
        P("ep", "tp"),
        P("ep", "tp"),
        P("ep", "tp"),
        P("ep", "tp"),
        P("ep", "tp"),
        P("tp"),
        P("tp", None),
        P("ep", None),
        P(),
        P("ep", None),
        P("ep"),
        P("ep", None),
        P("ep", None, "tp"),
        P("ep", None, "tp"),
        P("ep", "tp", None),
    )
    out_specs = (P(("ep", "tp"), None), P("ep", "tp"))
    return jax.shard_map(
        per_device, mesh=mesh, in_specs=in_specs, out_specs=out_specs, check_vma=False
    )
```
